32 devices in a mesh: sp: 8 (over z, y), tp: 4 (over x, core).
Axes of the slice: x: 2, y: 2, z: 4, core: 2. Of those that a mesh axis runs over, the one named last changes fastest.
Arguments:
- hidden_state: bfloat16 [1024, 2048], P('sp'), may hold values from -6 to 6
- out_grad: bfloat16 [1024, 2048], P('sp'), may hold values from -8 to 8
- routes: int32 [1024, 2], P('sp'), may hold values from 0 to 3, all different within a row; in each aligned block of 128 rows (0 to 127, 128 to 255, ...) at most 96 rows name the same one
- route_weights: float32 [1024, 2], P('sp'), may hold values from 0.25 to 1
- w_gate: bfloat16 [8, 2048, 1792], P('sp', None, 'tp'), may hold values from -0.125 to 0.125
- w_up: bfloat16 [8, 2048, 1792], P('sp', None, 'tp'), may hold values from -0.125 to 0.125
- w_down: bfloat16 [8, 1792, 2048], P('sp', 'tp'), may hold values from -0.09375 to 0.09375
- value: bfloat16 [1024, 512], P('sp', 'tp'), may hold values from -6 to 6
- gate_in: bfloat16 [1024, 512], P('sp', 'tp'), may hold values from -6 to 6
- normed: bfloat16 [1024, 512], P('sp', 'tp'), may hold values from -24 to 24
- inv_std: float32 [1024], P('sp'), may hold values from 0.5 to 2
- norm_gain: float32 [512], P('tp'), may hold values from 0.1 to 1.9
- taps: float32 [31, 512], P(None, 'tp'), may hold values from -1 to 1
- w_proj: bfloat16 [2048, 512], P(None, 'tp'), may hold values from -0.25 to 0.25
Outputs:
- w_gate_grad: bfloat16 [8, 2048, 1792], P('sp', None, 'tp')
- w_up_grad: bfloat16 [8, 2048, 1792], P('sp', None, 'tp')
- w_down_grad: bfloat16 [8, 1792, 2048], P('sp', 'tp')
- stream_grad: bfloat16 [1024, 2048], P('sp', 'tp')
- proj_grad: float32 [2048, 512], P('sp', 'tp')
- value_grad: bfloat16 [1024, 512], P('sp', 'tp')
- gate_in_grad: bfloat16 [1024, 512], P('sp', 'tp')
The draws below stay inside these ranges and needn't reach their ends.
Inputs may be any that keep to these rules, and one draw needn't show every extreme that they name: `routes`: among the choices of one device's tokens no expert is named more than 96 times, a bound that some block reaches on some device; a token's choices differ.
All inputs are finite; a program needn't handle non-finite values.
Results may differ from the reference program's by a relative error of at most 0.0057.
Values may be sent and summed in bfloat16 or wider, within the bound.
A program may use at most 128 MiB of HBM per device.

```python
import math
import jax
import jax.numpy as jnp
import numpy as np
from jax import lax

D = 2048
D_CH = 512
FF = 3584
KSIZE = 31
TOP = 2
GROUP = 2
TOK_DEV = 128
TOKENS = 1024
EXPERTS = 4
CAP = 96
N_SP = 8


def draw_normed(key, part):
    first_key, second_key, third_key = jax.random.split(key, 3)
    levels = jax.random.permutation(first_key, jnp.array([-0.7, 0.0, 0.7, 1.4], jnp.float32))
    spread = jax.random.uniform(second_key, (D_CH,), jnp.float32, -1.0, 1.0)
    channel_scale = jnp.exp(jnp.repeat(levels, D_CH // 4) + 0.3 * spread)
    base_values = jnp.clip(jax.random.normal(third_key, (TOKENS, D_CH), jnp.float32), -4.0, 4.0)
    return (base_values * channel_scale[None, :]).astype(jnp.bfloat16)


def strengthened(drawn, stream_key, source, target, parts, factor):
    owner, partner = [(jnp.arange(drawn.shape[dim]) // (drawn.shape[dim] // parts)).reshape([-1 if axis == dim else 1 for axis in range(drawn.ndim)]) for dim in (source, target)]
    chosen = jax.random.permutation(stream_key, parts)[partner]
    strong = (owner == chosen) | (owner == (partner + parts // 2) % parts)
    return jnp.where(strong, factor * drawn, drawn)


def level_of(key, shape, cuts, smallest, high):
    factor_of = 1.0
    for dim, blocks in cuts:
        heights = jax.random.uniform(jax.random.fold_in(jax.random.fold_in(key, 6), dim), (blocks,), jnp.float32, smallest / len(cuts), high / len(cuts))
        factor_of = factor_of * jnp.repeat(jnp.exp(heights), shape[dim] // blocks).reshape((-1,) + (1,) * (len(shape) - 1 - dim))
    return factor_of


def shared_out(stream_key, own, number, rows, count, top, bound, slope):
    order = jax.random.permutation(stream_key, count)
    heavy_load, common = portions_of(count, rows * top, bound, slope, True), portions_of(count, rows * top, bound, slope, False)
    places = jnp.arange(count)

    def named(tallies, offset_by):
        used = int((tallies > 0).sum())
        fixed = max(1, used // 4)
        passed = fixed + (places - fixed + offset_by * (used - fixed)) % max(1, count - fixed)
        return jnp.zeros((count,), jnp.int32).at[order[jnp.where(places < fixed, places, passed)]].set(jnp.asarray(tallies, jnp.int32))

    tallies = jnp.where(number % 4 == 0, named(heavy_load, number // 4), named(common, number - number // 4 - 1))
    mixed = jax.random.permutation(jax.random.fold_in(own, 3), count)
    giver, sink = mixed[0:count // 2 * 2:2], mixed[1:count // 2 * 2:2]
    margin = jnp.minimum(tallies[giver] - 1, bound - tallies[sink]) // 2
    margin = jnp.where((giver == order[0]) | (sink == order[0]) | (tallies[sink] == 0), 0, jnp.maximum(margin, 0))
    passed = jax.random.randint(jax.random.fold_in(own, 4), (count // 2,), 0, 1 << 20) % (margin + 1)
    tallies = tallies.at[giver].add(-passed).at[sink].add(passed)
    labels = jnp.searchsorted(jnp.cumsum(tallies), jnp.arange(rows * top), side="right").astype(jnp.int32)
    table = labels.reshape(top, rows).T
    table = table[jax.random.permutation(jax.random.fold_in(own, 1), rows)]
    offset_by = jax.random.randint(jax.random.fold_in(own, 2), (rows, 1), 0, top)
    return jnp.take_along_axis(table, (jnp.arange(top)[None, :] + offset_by) % top, axis=1)


def portions_of(count, total, reach, skew, full):
    weights = [(1 << 20) // math.isqrt(rank ** skew) + 1 for rank in range(1, count + 1)]
    largest = reach if full else min(reach, max(-(-total // count), total * weights[0] // sum(weights)))
    least = 1 if total - largest >= count - 1 else 0
    holding, surplus = [largest] + [least] * (count - 1), total - largest - least * (count - 1)
    while surplus > 0:
        free = [i for i in range(1, count) if holding[i] < largest] or [i for i in range(1, count) if holding[i] < reach]
        whole, remaining = sum([weights[i] for i in free]), surplus
        for i in free:
            extra = min(reach - holding[i], max(1, remaining * weights[i] // whole), surplus)
            holding[i] = holding[i] + extra
            surplus = surplus - extra
    return np.array(holding)


def scatter_about(key, extent, width, bound, pieces=(), kind=jnp.bfloat16):
    entries = width * jax.random.normal(key, extent, jnp.float32)
    if pieces:
        entries = entries * level_of(key, extent, pieces, -0.22, 0.18)
    return jnp.clip(entries, -bound, bound).astype(kind)


def noise_with(stream_key, extent, scale, limit, cuts, heavy, kind=jnp.bfloat16):
    values = scale * jax.random.normal(stream_key, extent, jnp.float32)
    if cuts:
        values = values * level_of(stream_key, extent, cuts, -0.22, 0.18)
    return jnp.clip(strengthened(values, jax.random.fold_in(stream_key, 3), *heavy), -limit, limit).astype(kind)


def setup_inputs(seed: int = 0) -> dict:
    seeds = jax.random.split(jax.random.key(seed), 15)
    hidden_state = scatter_about(seeds[0], (TOKENS, D), 1.0, 6.0, ((0, 8),))
    out_grad = noise_with(seeds[1], (TOKENS, D), 1.0, 8.0, ((0, 8),), (0, 1, 8, 2.0))
    routes_keys = jax.random.split(jax.random.fold_in(seeds[2], 1), TOKENS // TOK_DEV)
    routes_turns = jax.random.permutation(jax.random.fold_in(seeds[2], 3), TOKENS // TOK_DEV)
    routes = jax.vmap(lambda own, number: shared_out(jax.random.fold_in(seeds[2], 2), own, number, TOK_DEV, EXPERTS, TOP, CAP, 1))(routes_keys, routes_turns).reshape((TOKENS, TOP))
    route_weights = jnp.clip(0.25 + 0.75 * jax.random.uniform(seeds[3], (TOKENS, TOP), jnp.float32) ** level_of(seeds[3], (TOKENS, TOP), ((0, 8),), -0.2, 0.2), 0.25, 1.0)
    w_gate = scatter_about(seeds[4], (EXPERTS * GROUP, D, FF // GROUP), D ** -0.5, 0.125, ((0, 8), (2, 4)))
    w_up = scatter_about(seeds[5], (EXPERTS * GROUP, D, FF // GROUP), D ** -0.5, 0.125, ((0, 8), (2, 4)))
    w_down = scatter_about(seeds[6], (EXPERTS * GROUP, FF // GROUP, D), FF ** -0.5, 0.09375, ((0, 8), (1, 4)))
    value = scatter_about(seeds[7], (TOKENS, D_CH), 1.0, 6.0, ((0, 8), (1, 4)))
    gate_in = scatter_about(seeds[8], (TOKENS, D_CH), 1.0, 6.0, ((0, 8), (1, 4)))
    normed = draw_normed(jax.random.fold_in(seeds[14], 71), 0)
    inv_std = jnp.clip(jnp.exp(math.log(2.0) - 1.3862944 * jax.random.uniform(seeds[10], (TOKENS,), jnp.float32) ** level_of(seeds[10], (TOKENS,), ((0, 8),), -0.2, 0.2)), 0.5, 2.0)
    norm_gain = jnp.clip(1.0 + 0.18 * jax.random.normal(seeds[11], (D_CH,), jnp.float32), 0.1, 1.9)
    taps = scatter_about(seeds[12], (KSIZE, D_CH), 0.18, 1.0, ((1, 4),), jnp.float32)
    w_proj = scatter_about(seeds[13], (D, D_CH), D_CH ** -0.5, 0.25, ((1, 4),))
    return dict(hidden_state=hidden_state, out_grad=out_grad, routes=routes, route_weights=route_weights, w_gate=w_gate, w_up=w_up, w_down=w_down, value=value, gate_in=gate_in, normed=normed, inv_std=inv_std, norm_gain=norm_gain, taps=taps, w_proj=w_proj)


def expert_backward(in_rows, in_cots, gate_slice, up_slice, down_slice):
    pre_gate = jnp.dot(in_rows, gate_slice, preferred_element_type=jnp.float32)
    pre_up = jnp.dot(in_rows, up_slice, preferred_element_type=jnp.float32)
    gate_sig = jax.nn.sigmoid(pre_gate)
    silu_gate = pre_gate * gate_sig
    act_rows = (silu_gate * pre_up).astype(jnp.bfloat16)
    act_grad = lax.dot_general(in_cots, down_slice, (((1,), (1,)), ((), ())), preferred_element_type=jnp.float32)
    gate_grad = (act_grad * pre_up * gate_sig * (1.0 + pre_gate * (1.0 - gate_sig))).astype(jnp.bfloat16)
    up_grad = (act_grad * silu_gate).astype(jnp.bfloat16)
    down_grad = lax.dot_general(act_rows, in_cots, (((0,), (0,)), ((), ())), preferred_element_type=jnp.float32)
    gate_wgrad = lax.dot_general(in_rows, gate_grad, (((0,), (0,)), ((), ())), preferred_element_type=jnp.float32)
    up_wgrad = lax.dot_general(in_rows, up_grad, (((0,), (0,)), ((), ())), preferred_element_type=jnp.float32)
    row_grad = lax.dot_general(gate_grad, gate_slice, (((1,), (1,)), ((), ())), preferred_element_type=jnp.float32)
    row_grad = row_grad + lax.dot_general(up_grad, up_slice, (((1,), (1,)), ((), ())), preferred_element_type=jnp.float32)
    return gate_wgrad.astype(jnp.bfloat16), up_wgrad.astype(jnp.bfloat16), down_grad.astype(jnp.bfloat16), row_grad


def reference(hidden_state, out_grad, routes, route_weights, w_gate, w_up, w_down, value, gate_in, normed, inv_std, norm_gain, taps, w_proj):
    tokens, model_width = hidden_state.shape
    top_k = routes.shape[1]
    experts = N_SP // GROUP
    capacity = 3 * TOK_DEV * top_k // (2 * experts)
    per_dev = routes.reshape(N_SP, TOK_DEV * top_k).astype(jnp.int32)
    onehot = (per_dev[:, :, None] == jnp.arange(experts, dtype=jnp.int32)[None, None, :]).astype(jnp.int32)
    before = jnp.cumsum(onehot, axis=1) - onehot
    slot_index = jnp.sum(before * onehot, axis=2)
    source = jnp.arange(N_SP, dtype=jnp.int32)[:, None]
    slot_place = per_dev * (N_SP * capacity) + source * capacity + slot_index
    row_owner = source * TOK_DEV + jnp.arange(TOK_DEV * top_k, dtype=jnp.int32)[None, :] // top_k
    row_table = jnp.full((experts * N_SP * capacity,), tokens, jnp.int32)
    row_table = row_table.at[slot_place.reshape(-1)].set(row_owner.reshape(-1).astype(jnp.int32))
    row_table = row_table.reshape(experts, N_SP * capacity)
    row_scale = jnp.zeros((experts * N_SP * capacity,), jnp.float32)
    row_scale = row_scale.at[slot_place.reshape(-1)].set(route_weights.reshape(-1).astype(jnp.float32))
    row_scale = row_scale.reshape(experts, N_SP * capacity)
    zero_row = jnp.zeros((1, model_width), jnp.bfloat16)
    states = jnp.concatenate([hidden_state, zero_row], axis=0)
    cot_pad = jnp.concatenate([out_grad, zero_row], axis=0)

    def turn(row_total, slice_index):
        expert = (slice_index // GROUP).astype(jnp.int32)
        row_index = lax.dynamic_index_in_dim(row_table, expert, 0, False)
        scale_e = lax.dynamic_index_in_dim(row_scale, expert, 0, False)
        in_rows = jnp.take(states, row_index, axis=0)
        in_cots = (jnp.take(cot_pad, row_index, axis=0).astype(jnp.float32) * scale_e[:, None]).astype(jnp.bfloat16)
        gate_slice = lax.dynamic_index_in_dim(w_gate, slice_index, 0, False)
        up_slice = lax.dynamic_index_in_dim(w_up, slice_index, 0, False)
        down_slice = lax.dynamic_index_in_dim(w_down, slice_index, 0, False)
        gate_wgrad, up_wgrad, down_grad, row_grad = expert_backward(in_rows, in_cots, gate_slice, up_slice, down_slice)
        row_total = row_total.at[row_index].add(row_grad)
        return row_total, (gate_wgrad, up_wgrad, down_grad)

    row_total, weight_grads = lax.scan(turn, jnp.zeros((tokens + 1, model_width), jnp.float32), jnp.arange(experts * GROUP, dtype=jnp.int32))
    moe_grad = row_total[:tokens]
    stream_grad = (out_grad.astype(jnp.float32) + moe_grad).astype(jnp.bfloat16)
    proj_in = jnp.dot(stream_grad, w_proj, preferred_element_type=jnp.float32)
    saved_norm = normed.astype(jnp.float32)
    pre_act = saved_norm * norm_gain[None, :]
    act_sig = jax.nn.sigmoid(pre_act)
    silu_grad = proj_in * act_sig * (1.0 + pre_act * (1.0 - act_sig))
    norm_grad = silu_grad * norm_gain[None, :]
    mean_one = jnp.mean(norm_grad, axis=1, keepdims=True)
    mean_two = jnp.mean(norm_grad * saved_norm, axis=1, keepdims=True)
    conv_grad = inv_std[:, None] * (norm_grad - mean_one - saved_norm * mean_two)
    channels = conv_grad.shape[1]
    extended = jnp.concatenate([conv_grad, jnp.zeros((KSIZE - 1, channels), jnp.float32)], axis=0)
    glu_grad = taps[0][None, :] * extended[0:tokens]
    for tap_index in range(1, KSIZE):
        glu_grad = glu_grad + taps[tap_index][None, :] * extended[tap_index:tap_index + tokens]
    input_sig = jax.nn.sigmoid(gate_in.astype(jnp.float32))
    value_grad = (glu_grad * input_sig).astype(jnp.bfloat16)
    gate_in_grad = (glu_grad * value.astype(jnp.float32) * input_sig * (1.0 - input_sig)).astype(jnp.bfloat16)
    proj_act = (pre_act * act_sig).astype(jnp.bfloat16)
    proj_grad = lax.dot_general(stream_grad, proj_act, (((0,), (0,)), ((), ())), preferred_element_type=jnp.float32)
    return weight_grads[0], weight_grads[1], weight_grads[2], stream_grad, proj_grad, value_grad, gate_in_grad
```

```python
import functools

import jax
import jax.numpy as jnp
from jax import lax
from jax.experimental import pallas as pl
from jax.experimental.pallas import tpu as pltpu
from jax.sharding import PartitionSpec as P

GROUP = 2
PAIR = 2
MESH = pl.DeviceIdType.MESH
F32 = jnp.float32
BF16 = jnp.bfloat16


def dot_rows(a, b):
    return lax.dot_general(a, b, (((0,), (0,)), ((), ())), preferred_element_type=F32)


def dot_cols(a, b):
    return lax.dot_general(a, b, (((1,), (1,)), ((), ())), preferred_element_type=F32)


def place():
    s, t = lax.axis_index("sp"), lax.axis_index("tp")
    e, g = s // GROUP, s % GROUP
    hi, lo = t // PAIR, t % PAIR
    across = (s, (1 - hi) * PAIR + lo)
    beside = (e * GROUP + 1 - g, t)
    partner = (s, hi * PAIR + 1 - lo)
    return s, t, e, g, hi, lo, across, beside, partner


def greet(devices):
    barrier = pltpu.get_barrier_semaphore()
    for device in devices:
        pl.semaphore_signal(barrier, inc=1, device_id=device, device_id_type=MESH)
    pl.semaphore_wait(barrier, len(devices))


def remote(src, dst, send, recv, device):
    return pltpu.make_async_remote_copy(
        src_ref=src, dst_ref=dst, send_sem=send, recv_sem=recv, device_id=device, device_id_type=MESH
    )


def one_hot(rank_row, cap):
    slots = lax.broadcasted_iota(jnp.int32, (cap, rank_row.shape[1]), 0)
    return jnp.where(slots == rank_row, 1.0, 0.0)


def rank_tokens(routes_ref, weights_ref, rank_ref, w_ref):
    top, tok = routes_ref.shape
    experts = lax.broadcasted_iota(jnp.int32, rank_ref.shape, 0)
    named = jnp.zeros(rank_ref.shape, F32)
    weight = jnp.zeros(rank_ref.shape, F32)
    for k in range(top):
        hit = routes_ref[k : k + 1, :] == experts
        named = jnp.where(hit, 1.0, named)
        weight = jnp.where(hit, weights_ref[k : k + 1, :], weight)
    first = lax.broadcasted_iota(jnp.int32, (tok, tok), 0)
    second = lax.broadcasted_iota(jnp.int32, (tok, tok), 1)
    earlier = jnp.where(first < second, 1.0, 0.0).astype(BF16)
    rank = jnp.dot(named.astype(BF16), earlier, preferred_element_type=F32)
    rank_ref[...] = jnp.where(named > 0.0, rank, -1.0).astype(jnp.int32)
    w_ref[...] = weight


def mega_kernel(
    experts, cap, ksize,
    h_hbm, cot_hbm, routes_hbm, weights_hbm, gate_hbm, up_hbm, down_hbm,
    value_hbm, gin_hbm, normed_hbm, std_hbm, gain_hbm, taps_hbm, proj_hbm,
    gw, uw, dw, stream_ref, pgrad_ref, vgrad_ref, ggrad_ref,
    h_ref, cot_ref, routes_ref, weights_ref, value_ref, gate_ref, normed_ref, std_ref, gain_ref, taps_ref, proj_ref,
    rank_ref, w_ref, buf, pack, wg, wu, wd, act, gg, ug, flipped, grad_ref,
    from_core, sums, rx_a, ry_b, relay, rx2, back, done, full, stats, ext, pg, py, pz_out, pz,
    h_sem, w_sem, x_sem, d_send, d_recv, g_send, g_recv,
    core_send, core_recv, hop_send, hop_recv, z_send, z_recv, t_send, t_recv, p_send, p_recv, q_send, q_recv,
):
    s, t, e, g, hi, lo, across, beside, partner = place()
    sp_ways = experts * GROUP
    tok, quarter = cot_ref.shape
    half = quarter // 2
    tp_ways = stats.shape[0]
    across_t, other_t = across[1], partner[1]
    far_t = (1 - hi) * PAIR + 1 - lo
    far = (s, far_t)
    z_peers = [(lax.rem(e + j, experts) * GROUP + g, t) for j in range(1, experts)]
    before = (lax.rem(s + sp_ways - 1, sp_ways), t)
    after = (lax.rem(s + 1, sp_ways), t)
    cut = pl.ds(pl.multiple_of(t * quarter, quarter), quarter)

    def fetch(sem, *pairs):
        return [pltpu.make_async_copy(src, dst, sem.at[n]) for n, (src, dst) in enumerate(pairs)]

    takes = fetch(
        h_sem, (routes_hbm, routes_ref), (weights_hbm, weights_ref),
        (h_hbm.at[:, cut], h_ref), (cot_hbm.at[:, cut], cot_ref),
    )
    loads = fetch(w_sem, (gate_hbm, wg), (up_hbm, wu), (down_hbm, wd))
    extras = fetch(
        x_sem, (normed_hbm, normed_ref), (gain_hbm, gain_ref), (proj_hbm, proj_ref), (std_hbm, std_ref),
        (taps_hbm, taps_ref), (gin_hbm, gate_ref), (value_hbm, value_ref),
    )
    for copy in takes + loads + extras:
        copy.start()
    for copy in takes[:2]:
        copy.wait()
    rank_tokens(routes_ref, weights_ref, rank_ref, w_ref)
    for copy in takes[2:]:
        copy.wait()
    sent = []

    def go(copy):
        copy.start()
        sent.append(copy)

    def cols_of(col):
        return pl.ds(pl.multiple_of(col * quarter, quarter), quarter)

    def source_of(j):
        return lax.rem(e + experts - j, experts)

    def rows_of(j):
        return pl.ds(pl.multiple_of(j * GROUP * cap, cap), GROUP * cap)

    def loc(j, side, col):
        return pl.ds(pl.multiple_of((j * GROUP + side) * cap, cap), cap), cols_of(col)

    def d_copy(j):
        there, cols = loc(j, g, t)
        return remote(pack.at[j], buf.at[:, there, cols], d_send.at[j], d_recv.at[j], z_peers[j - 1])

    greeted = False
    for j in list(range(1, experts)) + [0]:
        target = lax.rem(e + j, experts)
        hot = one_hot(rank_ref[pl.ds(target, 1), :], cap)
        scale = jnp.sum(hot * w_ref[pl.ds(target, 1), :], axis=1, keepdims=True)
        hot = hot.astype(BF16)
        rows = jnp.dot(hot, h_ref[...], preferred_element_type=F32).astype(BF16)
        cots = (jnp.dot(hot, cot_ref[...], preferred_element_type=F32) * scale).astype(BF16)
        if j:
            pack[j, 0] = rows
            pack[j, 1] = cots
            if not greeted:
                greet(z_peers + [across, beside, partner, far, before, after])
                greeted = True
            go(d_copy(j))
        else:
            here, cols = loc(0, g, t)
            buf[0, here, cols] = rows
            buf[1, here, cols] = cots

    def hop(n, j, ref, device):
        return remote(ref, ref, g_send.at[j, n], g_recv.at[j, n], device)

    def both(j, side, col):
        rows, cols = loc(j, side, col)
        return buf.at[:, rows, cols]

    def one_of(k, j, side, col):
        rows, cols = loc(j, side, col)
        return buf.at[k, rows, cols]

    def arrived(n, j, ref):
        hop(n, j, ref, partner).wait_recv()

    def d_first(j):
        block = both(j, g, t)
        if j:
            remote(block, block, d_send.at[j], d_recv.at[j], partner).wait_recv()
        go(hop(0, j, block, across))
        go(hop(1, j, block, beside))
        go(hop(2, j, block, partner))

    def d_second(j):
        arrived(0, j, both(j, g, across_t))
        go(hop(3, j, one_of(0, j, g, across_t), beside))
        go(hop(5, j, both(j, g, across_t), partner))
        arrived(1, j, both(j, 1 - g, t))
        go(hop(4, j, one_of(1, j, 1 - g, t), across))
        go(hop(6, j, both(j, 1 - g, t), partner))

    def d_third(j):
        arrived(3, j, one_of(0, j, 1 - g, across_t))
        go(hop(7, j, one_of(0, j, 1 - g, across_t), partner))
        arrived(4, j, one_of(1, j, 1 - g, across_t))
        go(hop(8, j, one_of(1, j, 1 - g, across_t), partner))

    def d_last(j):
        arrived(2, j, both(j, g, other_t))
        arrived(5, j, both(j, g, far_t))
        arrived(6, j, both(j, 1 - g, other_t))
        arrived(7, j, one_of(0, j, 1 - g, far_t))
        arrived(8, j, one_of(1, j, 1 - g, far_t))

    def compute(j):
        rows = rows_of(j)
        in_rows = buf[0, rows, :]
        in_cots = buf[1, rows, :]
        pre_gate = dot_cols(in_rows, wg[...])
        pre_up = dot_cols(in_rows, wu[...])
        gate_sig = jax.nn.sigmoid(pre_gate)
        silu_gate = pre_gate * gate_sig
        act_grad = dot_cols(in_cots, wd[...])
        gate_grad = (act_grad * pre_up * gate_sig * (1.0 + pre_gate * (1.0 - gate_sig))).astype(BF16)
        up_grad = (act_grad * silu_gate).astype(BF16)
        act[rows, :] = (silu_gate * pre_up).astype(BF16)
        gg[rows, :] = gate_grad
        ug[rows, :] = up_grad
        grad_ref[rows, :] = (
            jnp.dot(gate_grad, wg[...], preferred_element_type=F32) + jnp.dot(up_grad, wu[...], preferred_element_type=F32)
        ).astype(BF16)

    width = full.shape[1]
    piece = 256
    per_item = width // piece // 4

    def weight_item(which, n):
        if n == 0:
            flipped[...] = (gg, ug, act)[which][...].T

        @pl.loop(n * per_item, (n + 1) * per_item)
        def _(i):
            cols = pl.ds(pl.multiple_of(i * piece, piece), piece)
            rows = buf[1 if which == 2 else 0, :, cols]
            (gw, uw, dw)[which][:, cols] = jnp.dot(flipped[...], rows, preferred_element_type=F32).astype(BF16)

    items = [(which, n) for which in range(3) for n in range(4)]

    def fill(count=1):
        for _ in range(count):
            if items:
                which, n = items.pop(0)
                weight_item(which, n)

    def core_copy(j, h, lane):
        return remote(
            grad_ref.at[rows_of(j), cols_of(h * PAIR + lane)],
            from_core.at[j, h], core_send.at[j, h], core_recv.at[j, h], partner,
        )

    def hop_copy(n, j, src, dst, device):
        return remote(src, dst, hop_send.at[j, n], hop_recv.at[j, n], device)

    def x_first(j):
        return hop_copy(0, j, sums.at[0, j, 1 - hi], rx_a.at[j], across)

    def y_first(j):
        return hop_copy(1, j, sums.at[1, j, :, 1 - g], ry_b.at[j], beside)

    def y_second(j):
        return hop_copy(2, j, relay.at[0, j], rx2.at[0, j], beside)

    def x_second(j):
        return hop_copy(3, j, relay.at[1, j], rx2.at[1, j], across)

    def z_copy(j):
        return remote(done.at[j], back.at[j], z_send.at[j], z_recv.at[j], (source_of(j) * GROUP + g, t))

    def first(j):
        for h in range(PAIR):
            core_copy(j, h, lo).wait_recv()
            mine = grad_ref[rows_of(j), cols_of(h * PAIR + lo)].astype(F32)
            total = (mine + from_core[j, h].astype(F32)).astype(BF16).reshape(GROUP, cap, quarter)
            sums[0, j, h] = total[:, :, :half]
            sums[1, j, h] = total[:, :, half:]
        go(x_first(j))
        go(y_first(j))

    def second(j):
        x_first(j).wait_recv()
        relay[0, j] = (sums[0, j, hi, 1 - g].astype(F32) + rx_a[j, 1 - g].astype(F32)).astype(BF16)
        go(y_second(j))
        y_first(j).wait_recv()
        relay[1, j] = (sums[1, j, 1 - hi, g].astype(F32) + ry_b[j, 1 - hi].astype(F32)).astype(BF16)
        go(x_second(j))

    def third(j):
        y_second(j).wait_recv()
        done[j, :, :half] = (
            sums[0, j, hi, g].astype(F32) + rx_a[j, g].astype(F32) + rx2[0, j].astype(F32)
        ).astype(BF16)
        x_second(j).wait_recv()
        done[j, :, half:] = (
            sums[1, j, hi, g].astype(F32) + ry_b[j, hi].astype(F32) + rx2[1, j].astype(F32)
        ).astype(BF16)
        if j:
            go(z_copy(j))

    step = max(1, experts // 4)
    chunks = [list(range(c, min(c + step, experts))) for c in range(0, experts, step)]

    def returns(c, fills):
        for stage, lag in ((first, 1), (second, 2), (third, 3)):
            if 0 <= c - lag < len(chunks):
                for j in chunks[c - lag]:
                    stage(j)
                fill(fills)

    for i in range(experts + 3):
        if i < experts:
            d_first(i)
        if 0 <= i - 1 < experts:
            d_second(i - 1)
        if 0 <= i - 2 < experts:
            d_third(i - 2)
        j = i - 3
        if j >= 0:
            if j == 0:
                for copy in loads:
                    copy.wait()
            d_last(j)
            if j % step == step - 1 or j == experts - 1:
                c = j // step
                if len(chunks[c]) == 1:
                    compute(j)
                else:
                    pl.loop(chunks[c][0], chunks[c][-1] + 1)(compute)
                for k in chunks[c]:
                    for h in range(PAIR):
                        go(core_copy(k, h, 1 - lo))
                returns(c, 1 if c == len(chunks) - 1 else 0)
    for c in range(len(chunks), len(chunks) + 3):
        returns(c, 1)
    fill(len(items))

    for copy in extras:
        copy.wait()
    gain = gain_ref[...]
    saved = normed_ref[...].astype(F32)
    pre_act = saved * gain
    act_sig = jax.nn.sigmoid(pre_act)
    slope = act_sig * (1.0 + pre_act * (1.0 - act_sig))
    proj_act = (pre_act * act_sig).astype(BF16)

    stream = cot_ref[...].astype(F32)
    for j in [0] + list(range(1, experts)):
        if j:
            z_copy(j).wait_recv()
            block = back[j]
        else:
            block = done[0]
        source = lax.rem(e + j, experts)
        hot = one_hot(rank_ref[pl.ds(source, 1), :], cap).astype(BF16)
        stream = stream + dot_rows(hot, block)
    stream = stream.astype(BF16)
    stream_ref[...] = stream
    full[:, cols_of(t)] = stream

    def gather_copy(n, col, device):
        return remote(full.at[:, cols_of(col)], full.at[:, cols_of(col)], t_send.at[n], t_recv.at[n], device)

    go(gather_copy(0, t, across))
    go(gather_copy(1, t, partner))
    gather_copy(0, across[1], across).wait_recv()
    go(gather_copy(2, across[1], partner))
    gather_copy(1, partner[1], partner).wait_recv()
    gather_copy(2, far[1], partner).wait_recv()

    rows = pg.shape[2]

    def p_copy(j):
        return remote(pg.at[j, 1 - g], py.at[j], p_send.at[j], p_recv.at[j], beside)

    whole = dot_rows(full[...], proj_act)
    pall = whole.reshape(experts, GROUP, rows, whole.shape[1])
    for i in range(experts):
        pg[i] = pall[i].astype(BF16)
    for i in range(experts):
        go(p_copy(i))

    proj_in = jnp.dot(full[...], proj_ref[...], preferred_element_type=F32)
    norm_grad = proj_in * slope * gain
    one = jnp.sum(norm_grad, axis=1, keepdims=True)
    two = jnp.sum(norm_grad * saved, axis=1, keepdims=True)
    lane = lax.broadcasted_iota(jnp.int32, (tok, 128), 1)
    packed = jnp.where(lane == 0, one, jnp.where(lane == 1, two, 0.0))
    stats[t] = packed.T[:8]

    def stat_copy(n, device, owner):
        return remote(stats.at[owner], stats.at[owner], t_send.at[n], t_recv.at[n], device)

    for n, device in ((3, across), (4, far), (5, partner)):
        go(stat_copy(n, device, t))

    def q_copy(j):
        return remote(pz_out.at[j], pz.at[j], q_send.at[j], q_recv.at[j], z_peers[j - 1])

    for n, device in ((3, across), (4, far), (5, partner)):
        stat_copy(n, device, device[1]).wait_recv()
    total = stats[0]
    for i in range(1, tp_ways):
        total = total + stats[i]
    total = jnp.concatenate([total, jnp.zeros((120, tok), F32)], axis=0).T
    channels = saved.shape[1] * tp_ways
    mean_one = total[:, 0:1] / channels
    mean_two = total[:, 1:2] / channels
    std = jnp.broadcast_to(std_ref[...], (tok, tok)).T[:, 0:1]
    conv = std * (norm_grad - mean_one - saved * mean_two)
    ext[pl.ds(0, tok), :] = conv

    def halo_copy():
        return remote(ext.at[pl.ds(0, 32)], ext.at[pl.ds(tok, 32)], t_send.at[6], t_recv.at[6], before)

    @pl.when(s > 0)
    def _():
        halo_copy().start()

    for i in range(experts):
        p_copy(i).wait_recv()
    for j in list(range(1, experts)) + [0]:
        target = lax.rem(e + j, experts)
        piece = pg[target, g].astype(F32) + py[target].astype(F32)
        if j:
            pz_out[j] = piece.astype(BF16)
            go(q_copy(j))
        else:
            pgrad_ref[...] = piece

    @pl.when(s < sp_ways - 1)
    def _():
        halo_copy().wait_recv()

    @pl.when(s == sp_ways - 1)
    def _():
        ext[pl.ds(tok, 32), :] = jnp.zeros((32, ext.shape[1]), F32)

    glu = taps_ref[0:1, :] * ext[pl.ds(0, tok), :]
    for k in range(1, ksize):
        glu = glu + taps_ref[k : k + 1, :] * ext[pl.ds(k, tok), :]
    in_sig = jax.nn.sigmoid(gate_ref[...].astype(F32))
    vgrad_ref[...] = (glu * in_sig).astype(BF16)
    ggrad_ref[...] = (glu * value_ref[...].astype(F32) * in_sig * (1.0 - in_sig)).astype(BF16)

    total = pgrad_ref[...]
    for j in range(1, experts):
        q_copy(j).wait_recv()
        total = total + pz[j].astype(F32)
    pgrad_ref[...] = total

    @pl.when(s > 0)
    def _():
        halo_copy().wait_send()

    for copy in sent:
        copy.wait_send()


def mega(hidden, cot, routes, weights, w_gate, w_up, w_down, value, gate_in, normed, std, gain, taps, w_proj, experts, cap, tp_ways):
    vmem = pl.BlockSpec(memory_space=pltpu.VMEM)
    hbm = pl.BlockSpec(memory_space=pl.ANY)
    tok, width = cot.shape
    units = w_gate.shape[0]
    quarter = width // tp_ways
    padded = -(-experts // 8) * 8
    total = experts * GROUP * cap
    ch = normed.shape[1]
    rows = width // (experts * GROUP)
    half = quarter // 2
    dma = pltpu.SemaphoreType.DMA
    arrays = (hidden, cot, routes, weights, w_gate, w_up, w_down, value, gate_in, normed, std, gain, taps, w_proj)
    assert taps.shape[0] - 1 <= 32
    return pl.pallas_call(
        functools.partial(mega_kernel, experts, cap, taps.shape[0]),
        out_shape=(
            pltpu.VMEM((units, width), BF16),
            pltpu.VMEM((units, width), BF16),
            pltpu.VMEM((units, width), BF16),
            pltpu.VMEM((tok, quarter), BF16),
            pltpu.VMEM((rows, ch), F32),
            pltpu.VMEM((tok, ch), BF16),
            pltpu.VMEM((tok, ch), BF16),
        ),
        in_specs=[hbm] * len(arrays),
        out_specs=(vmem,) * 7,
        scratch_shapes=[
            pltpu.VMEM((tok, quarter), BF16),
            pltpu.VMEM((tok, quarter), BF16),
            *[pltpu.VMEM(a.shape, a.dtype) for a in (routes, weights, value, gate_in, normed, std, gain, taps, w_proj)],
            pltpu.VMEM((padded, tok), jnp.int32),
            pltpu.VMEM((padded, tok), F32),
            pltpu.VMEM((2, total, width), BF16),
            pltpu.VMEM((experts, 2, cap, quarter), BF16),
            pltpu.VMEM((units, width), BF16),
            pltpu.VMEM((units, width), BF16),
            pltpu.VMEM((units, width), BF16),
            pltpu.VMEM((total, units), BF16),
            pltpu.VMEM((total, units), BF16),
            pltpu.VMEM((total, units), BF16),
            pltpu.VMEM((units, total), BF16),
            pltpu.VMEM((total, width), BF16),
            pltpu.VMEM((experts, PAIR, GROUP * cap, quarter), BF16),
            pltpu.VMEM((2, experts, PAIR, GROUP, cap, half), BF16),
            pltpu.VMEM((experts, GROUP, cap, half), BF16),
            pltpu.VMEM((experts, PAIR, cap, half), BF16),
            pltpu.VMEM((2, experts, cap, half), BF16),
            pltpu.VMEM((2, experts, cap, half), BF16),
            pltpu.VMEM((experts, cap, quarter), BF16),
            pltpu.VMEM((experts, cap, quarter), BF16),
            pltpu.VMEM((tok, width), BF16),
            pltpu.VMEM((tp_ways, 8, tok), F32),
            pltpu.VMEM((tok + 32, ch), F32),
            pltpu.VMEM((experts, GROUP, rows, ch), BF16),
            pltpu.VMEM((experts, rows, ch), BF16),
            pltpu.VMEM((experts, rows, ch), BF16),
            pltpu.VMEM((experts, rows, ch), BF16),
            dma((4,)),
            dma((3,)),
            dma((7,)),
            dma((experts,)),
            dma((experts,)),
            dma((experts, 9)),
            dma((experts, 9)),
            dma((experts, PAIR)),
            dma((experts, PAIR)),
            dma((experts, 4)),
            dma((experts, 4)),
            dma((experts,)),
            dma((experts,)),
            dma((7,)),
            dma((7,)),
            dma((experts,)),
            dma((experts,)),
            dma((experts,)),
            dma((experts,)),
        ],
        compiler_params=pltpu.CompilerParams(
            collective_id=0, has_side_effects=True, vmem_limit_bytes=44 * 1024 * 1024
        ),
        name="mega",
    )(*[pltpu.with_memory_space_constraint(a, pltpu.HBM) for a in arrays])


def finish_kernel(count, *refs):
    copies = [pltpu.make_async_copy(refs[n], refs[count + n], refs[-1].at[n]) for n in range(count)]
    for copy in copies:
        copy.start()
    for copy in copies:
        copy.wait()


def finish(*arrays):
    count = len(arrays)
    return pl.pallas_call(
        functools.partial(finish_kernel, count),
        out_shape=tuple(jax.ShapeDtypeStruct(a.shape, a.dtype) for a in arrays),
        in_specs=[pl.BlockSpec(memory_space=pltpu.VMEM)] * count,
        out_specs=(pl.BlockSpec(memory_space=pl.ANY),) * count,
        scratch_shapes=[pltpu.SemaphoreType.DMA((count,))],
        compiler_params=pltpu.CompilerParams(vmem_limit_bytes=8 * 1024 * 1024),
        name="finish",
    )(*[pltpu.with_memory_space_constraint(a, pltpu.VMEM) for a in arrays])


def on_device(
    hidden_state, out_grad, routes, route_weights, w_gate, w_up, w_down,
    value, gate_in, normed, inv_std, norm_gain, taps, w_proj,
):
    tok = hidden_state.shape[0]
    top_k = routes.shape[1]
    sp_ways, tp_ways = lax.axis_size("sp"), lax.axis_size("tp")
    experts = sp_ways // GROUP
    cap = 3 * tok * top_k // (2 * experts)
    cap = -(-cap // 16) * 16
    results = mega(
        hidden_state, out_grad, routes.T, route_weights.T, w_gate[0].T, w_up[0].T, w_down[0], value, gate_in, normed,
        inv_std[None, :], norm_gain[None, :], taps, w_proj, experts, cap, tp_ways,
    )
    gate_wgrad, up_wgrad, down_grad, stream_part, proj_grad, value_grad, gate_in_grad = finish(*results)
    return gate_wgrad.T[None], up_wgrad.T[None], down_grad[None], stream_part, proj_grad, value_grad, gate_in_grad


def solution(mesh):
    in_specs = (
        P("sp", None), P("sp", None), P("sp", None), P("sp", None),
        P("sp", None, "tp"), P("sp", None, "tp"), P("sp", "tp", None),
        P("sp", "tp"), P("sp", "tp"), P("sp", "tp"), P("sp"), P("tp"), P(None, "tp"), P(None, "tp"),
    )
    out_specs = (
        P("sp", None, "tp"), P("sp", None, "tp"), P("sp", "tp", None),
        P("sp", "tp"), P("sp", "tp"), P("sp", "tp"), P("sp", "tp"),
    )
    return jax.shard_map(on_device, mesh=mesh, in_specs=in_specs, out_specs=out_specs, check_vma=False)
```

```python
import functools

import jax
import jax.numpy as jnp
from jax import lax
from jax.experimental import pallas as pl
from jax.experimental.pallas import tpu as pltpu
from jax.sharding import PartitionSpec as P

GROUP = 2
PAIR = 2
MESH = pl.DeviceIdType.MESH
F32 = jnp.float32
BF16 = jnp.bfloat16


def dot_rows(a, b):
    return lax.dot_general(a, b, (((0,), (0,)), ((), ())), preferred_element_type=F32)


def dot_cols(a, b):
    return lax.dot_general(a, b, (((1,), (1,)), ((), ())), preferred_element_type=F32)


def place():
    s, t = lax.axis_index("sp"), lax.axis_index("tp")
    e, g = s // GROUP, s % GROUP
    hi, lo = t // PAIR, t % PAIR
    across = (s, (1 - hi) * PAIR + lo)
    beside = (e * GROUP + 1 - g, t)
    partner = (s, hi * PAIR + 1 - lo)
    return s, t, e, g, hi, lo, across, beside, partner


def flip(place, bits):
    bit = 1
    while bit <= bits:
        if bits & bit:
            place = place + bit - 2 * bit * lax.rem(place // bit, 2)
        bit *= 2
    return place


def greet(devices):
    barrier = pltpu.get_barrier_semaphore()
    for device in devices:
        pl.semaphore_signal(barrier, inc=1, device_id=device, device_id_type=MESH)
    pl.semaphore_wait(barrier, len(devices))


def remote(src, dst, send, recv, device):
    return pltpu.make_async_remote_copy(
        src_ref=src, dst_ref=dst, send_sem=send, recv_sem=recv, device_id=device, device_id_type=MESH
    )


def one_hot(rank_row, cap):
    slots = lax.broadcasted_iota(jnp.int32, (cap, rank_row.shape[1]), 0)
    return jnp.where(slots == rank_row, 1.0, 0.0)


def rank_tokens(routes_ref, weights_ref, rank_ref, w_ref):
    top, tok = routes_ref.shape
    experts = lax.broadcasted_iota(jnp.int32, rank_ref.shape, 0)
    named = jnp.zeros(rank_ref.shape, F32)
    weight = jnp.zeros(rank_ref.shape, F32)
    for k in range(top):
        hit = routes_ref[k : k + 1, :] == experts
        named = jnp.where(hit, 1.0, named)
        weight = jnp.where(hit, weights_ref[k : k + 1, :], weight)
    first = lax.broadcasted_iota(jnp.int32, (tok, tok), 0)
    second = lax.broadcasted_iota(jnp.int32, (tok, tok), 1)
    earlier = jnp.where(first < second, 1.0, 0.0).astype(BF16)
    rank = jnp.dot(named.astype(BF16), earlier, preferred_element_type=F32)
    rank_ref[...] = jnp.where(named > 0.0, rank, -1.0).astype(jnp.int32)
    w_ref[...] = weight


def mega_kernel(
    experts, cap, ksize,
    h_hbm, cot_hbm, routes_hbm, weights_hbm, gate_hbm, up_hbm, down_hbm,
    value_hbm, gin_hbm, normed_hbm, std_hbm, gain_hbm, taps_hbm, proj_hbm,
    gw, uw, dw, stream_ref, pgrad_ref, vgrad_ref, ggrad_ref,
    h_ref, cot_ref, routes_ref, weights_ref, value_ref, gate_ref, normed_ref, std_ref, gain_ref, taps_ref, proj_ref,
    rank_ref, w_ref, buf, pack, wg, wu, wd, act, gg, ug, flipped, grad_ref,
    from_core, sums, rx_a, ry_b, relay, rx2, back, done, full, stats, ext, pg, py, pz_out, pz,
    h_sem, w_sem, x_sem, l_send, l_recv, c_send, c_recv,
    core_send, core_recv, hop_send, hop_recv, z_send, z_recv, t_send, t_recv, p_send, p_recv, q_send, q_recv,
):
    s, t, e, g, hi, lo, across, beside, partner = place()
    sp_ways = experts * GROUP
    tp_ways = stats.shape[0]
    tok, quarter = cot_ref.shape[0], cot_ref.shape[1] // tp_ways
    half = quarter // 2
    across_t, other_t = across[1], partner[1]
    far_t = (1 - hi) * PAIR + 1 - lo
    far = (s, far_t)
    planes = [flip(e, j) for j in range(experts)]
    z_peers = [(planes[j] * GROUP + g, t) for j in range(1, experts)]
    before = (lax.rem(s + sp_ways - 1, sp_ways), t)
    after = (lax.rem(s + 1, sp_ways), t)
    def fetch(sem, *pairs):
        return [pltpu.make_async_copy(src, dst, sem.at[n]) for n, (src, dst) in enumerate(pairs)]

    takes = fetch(
        h_sem, (routes_hbm, routes_ref), (weights_hbm, weights_ref),
        (h_hbm, h_ref), (cot_hbm, cot_ref),
    )
    loads = fetch(w_sem, (gate_hbm, wg), (up_hbm, wu), (down_hbm, wd))
    extras = fetch(
        x_sem, (normed_hbm, normed_ref), (gain_hbm, gain_ref), (proj_hbm, proj_ref), (std_hbm, std_ref),
        (taps_hbm, taps_ref), (gin_hbm, gate_ref), (value_hbm, value_ref),
    )
    for copy in takes:
        copy.start()
    for copy in takes[:2]:
        copy.wait()
    rank_tokens(routes_ref, weights_ref, rank_ref, w_ref)
    for copy in takes[2:]:
        copy.wait()
    for copy in loads + extras:
        copy.start()
    sent = []

    def go(copy):
        copy.start()
        sent.append(copy)

    def cols_of(col):
        return pl.ds(pl.multiple_of(col * quarter, quarter), quarter)

    def rows_of(j):
        return pl.ds(pl.multiple_of(j * GROUP * cap, cap), GROUP * cap)

    def loc(j, side, col):
        return pl.ds(pl.multiple_of((j * GROUP + side) * cap, cap), cap), cols_of(col)

    def chosen(j):
        plane = pl.ds(planes[j], 1)
        hot = one_hot(rank_ref[plane, :], cap)
        return hot.astype(BF16), jnp.sum(hot * w_ref[plane, :], axis=1, keepdims=True)

    sides = (g, 1 - g)
    spread = (t, across_t)

    def spot(k, j, side, col):
        rows, cols = loc(j, sides[side], spread[col])
        return buf.at[k, rows, cols]

    def link(k, j, side, col, src, dst, device):
        return remote(src, dst, l_send.at[j, k, side, col], l_recv.at[j, k, side, col], device)

    def landed(k, j, side, col):
        ref = spot(k, j, side, col)
        link(k, j, side, col, ref, ref, partner).wait_recv()

    def pass_on(k, j, side, col, src, device):
        ref = spot(k, j, *src)
        go(link(k, j, side, col, ref, ref, device))

    def core(j, side, col):
        rows, cols = loc(j, sides[side], spread[col])
        ref = buf.at[:, rows, cols]
        return remote(ref, ref, c_send.at[j, side, col], c_recv.at[j, side, col], partner)

    def core_landed(j, side, col):
        rows, cols = loc(j, sides[side], (other_t, far_t)[col])
        ref = buf.at[:, rows, cols]
        remote(ref, ref, c_send.at[j, side, col], c_recv.at[j, side, col], partner).wait_recv()

    step = max(1, experts // 4)
    blocks = [list(range(c, min(c + step, experts))) for c in range(0, experts, step)]
    first_block, last_blocks = blocks[1], blocks[:1:-1]
    outer = [j for block in [first_block] + last_blocks + blocks[:1] for j in block if j]
    for n, j in enumerate(outer):
        hot, scale = chosen(j)
        pack[j, 0] = jnp.dot(hot, h_ref[:, cols_of(t)], preferred_element_type=F32).astype(BF16)
        pack[j, 1] = (jnp.dot(hot, cot_ref[:, cols_of(t)], preferred_element_type=F32) * scale).astype(BF16)
        if not n:
            greet(z_peers + [across, beside, partner, far, before, after])
        for k in range(2):
            go(link(k, j, 0, 0, pack.at[j, k], spot(k, j, 0, 0), z_peers[j - 1]))
    hot, scale = chosen(0)
    here = loc(0, g, t)[0]
    buf[0, here, :] = jnp.dot(hot, h_ref[...], preferred_element_type=F32).astype(BF16)
    buf[1, here, :] = (jnp.dot(hot, cot_ref[...], preferred_element_type=F32) * scale).astype(BF16)

    def d_first(j):
        for k in range(2):
            if j:
                landed(k, j, 0, 0)
                pass_on(k, j, 0, 1, (0, 0), across)
            pass_on(k, j, 1, 0, (0, 0), beside)
        if j:
            go(core(j, 0, 0))

    def d_second(j):
        if j:
            landed(0, j, 0, 1)
            pass_on(0, j, 1, 1, (0, 1), beside)
            landed(1, j, 1, 0)
            pass_on(1, j, 1, 1, (1, 0), across)
            landed(1, j, 0, 1)
            go(core(j, 0, 1))
            landed(0, j, 1, 0)
        else:
            for k in range(2):
                landed(k, j, 1, 0)
                pass_on(k, j, 1, 1, (1, 0), across)
        go(core(j, 1, 0))

    def d_third(j):
        for k in range(2):
            landed(k, j, 1, 1)
        go(core(j, 1, 1))

    def d_last(j):
        for side in range(0 if j else 1, 2):
            for col in range(2):
                core_landed(j, side, col)

    def compute(j):
        rows = rows_of(j)
        in_rows = buf[0, rows, :]
        in_cots = buf[1, rows, :]
        pre_gate = dot_cols(in_rows, wg[...])
        pre_up = dot_cols(in_rows, wu[...])
        gate_sig = jax.nn.sigmoid(pre_gate)
        silu_gate = pre_gate * gate_sig
        act_grad = dot_cols(in_cots, wd[...])
        gate_grad = (act_grad * pre_up * gate_sig * (1.0 + pre_gate * (1.0 - gate_sig))).astype(BF16)
        up_grad = (act_grad * silu_gate).astype(BF16)
        act[rows, :] = (silu_gate * pre_up).astype(BF16)
        gg[rows, :] = gate_grad
        ug[rows, :] = up_grad
        for lane in (1 - lo, lo):
            for h in range(PAIR):
                cols = cols_of(h * PAIR + lane)
                grad_ref[rows, cols] = (
                    jnp.dot(gate_grad, wg[:, cols], preferred_element_type=F32)
                    + jnp.dot(up_grad, wu[:, cols], preferred_element_type=F32)
                ).astype(BF16)
                if lane is not lo and isinstance(j, int):
                    go(core_copy(j, h, 1 - lo))

    width = full.shape[1]
    piece = 256
    per_item = width // piece // 4

    def weight_item(which, n):
        if n == 0:
            flipped[...] = (gg, ug, act)[which][...].T

        @pl.loop(n * per_item, (n + 1) * per_item)
        def _(i):
            cols = pl.ds(pl.multiple_of(i * piece, piece), piece)
            rows = buf[1 if which == 2 else 0, :, cols]
            (gw, uw, dw)[which][:, cols] = jnp.dot(flipped[...], rows, preferred_element_type=F32).astype(BF16)

    items = [(which, n) for which in range(3) for n in range(4)]

    def fill(count=1):
        for _ in range(count):
            if items:
                which, n = items.pop(0)
                weight_item(which, n)

    def core_copy(j, h, lane):
        return remote(
            grad_ref.at[rows_of(j), cols_of(h * PAIR + lane)],
            from_core.at[j, h], core_send.at[j, h], core_recv.at[j, h], partner,
        )

    def hop_copy(n, j, src, dst, device):
        return remote(src, dst, hop_send.at[j, n], hop_recv.at[j, n], device)

    def x_first(j):
        return hop_copy(0, j, sums.at[0, j, 1 - hi], rx_a.at[j], across)

    def y_first(j):
        return hop_copy(1, j, sums.at[1, j, :, 1 - g], ry_b.at[j], beside)

    def y_second(j):
        return hop_copy(2, j, relay.at[0, j], rx2.at[0, j], beside)

    def x_second(j):
        return hop_copy(3, j, relay.at[1, j], rx2.at[1, j], across)

    def z_copy(j):
        return remote(done.at[j], back.at[j], z_send.at[j], z_recv.at[j], z_peers[j - 1])

    def first(j):
        for h in range(PAIR):
            core_copy(j, h, lo).wait_recv()
            mine = grad_ref[rows_of(j), cols_of(h * PAIR + lo)].astype(F32)
            total = (mine + from_core[j, h].astype(F32)).astype(BF16).reshape(GROUP, cap, quarter)
            sums[0, j, h] = total[:, :, :half]
            sums[1, j, h] = total[:, :, half:]
        go(x_first(j))
        go(y_first(j))

    def second(j):
        x_first(j).wait_recv()
        relay[0, j] = (sums[0, j, hi, 1 - g].astype(F32) + rx_a[j, 1 - g].astype(F32)).astype(BF16)
        go(y_second(j))
        y_first(j).wait_recv()
        relay[1, j] = (sums[1, j, 1 - hi, g].astype(F32) + ry_b[j, 1 - hi].astype(F32)).astype(BF16)
        go(x_second(j))

    def third(j):
        y_second(j).wait_recv()
        done[j, :, :half] = (
            sums[0, j, hi, g].astype(F32) + rx_a[j, g].astype(F32) + rx2[0, j].astype(F32)
        ).astype(BF16)
        x_second(j).wait_recv()
        done[j, :, half:] = (
            sums[1, j, hi, g].astype(F32) + ry_b[j, hi].astype(F32) + rx2[1, j].astype(F32)
        ).astype(BF16)
        if j:
            go(z_copy(j))

    def flow(*stages):
        for stage, block in stages:
            for j in block:
                stage(j)

    def work(block):
        if len(block) == 1:
            compute(block[0])
            return
        pl.loop(block[0], block[-1] + 1)(compute)
        for j in block:
            for h in range(PAIR):
                go(core_copy(j, h, 1 - lo))

    own, near, far_one, far_two = blocks[0], first_block, *last_blocks
    d_first(0)
    flow((d_first, near), (d_second, near), (d_first, own[1:]), (d_second, own), (d_third, near))
    flow((d_last, near), (d_first, far_one))
    for copy in loads:
        copy.wait()
    work(near)
    flow((d_third, own), (d_first, far_two), (d_last, own))
    work(own)
    flow((d_second, far_one), (d_second, far_two), (first, near), (first, own), (d_third, far_one), (d_last, far_one))
    work(far_one)
    flow((d_third, far_two), (first, far_one), (d_last, far_two), (second, near), (second, own))
    work(far_two)
    flow((first, far_two))
    fill(1)
    flow((second, far_one))
    fill(1)
    flow((third, near))
    fill(1)
    flow((third, own))
    fill(1)
    flow((second, far_two))
    fill(2)
    flow((third, far_one))
    fill(1)
    flow((third, far_two))
    fill(len(items))

    for copy in extras:
        copy.wait()
    gain = gain_ref[...]
    saved = normed_ref[...].astype(F32)
    pre_act = saved * gain
    act_sig = jax.nn.sigmoid(pre_act)
    slope = act_sig * (1.0 + pre_act * (1.0 - act_sig))
    proj_act = (pre_act * act_sig).astype(BF16)

    stream = cot_ref[:, cols_of(t)].astype(F32)
    for j in [0] + list(range(1, experts)):
        if j:
            z_copy(j).wait_recv()
            block = back[j]
        else:
            block = done[0]
        hot = one_hot(rank_ref[pl.ds(planes[j], 1), :], cap).astype(BF16)
        stream = stream + dot_rows(hot, block)
    stream = stream.astype(BF16)
    stream_ref[...] = stream
    full[:, cols_of(t)] = stream

    def gather_copy(n, col, device):
        return remote(full.at[:, cols_of(col)], full.at[:, cols_of(col)], t_send.at[n], t_recv.at[n], device)

    go(gather_copy(0, t, across))
    go(gather_copy(1, t, partner))
    gather_copy(0, across[1], across).wait_recv()
    go(gather_copy(2, across[1], partner))
    gather_copy(1, partner[1], partner).wait_recv()
    gather_copy(2, far[1], partner).wait_recv()

    rows = pg.shape[2]

    def p_copy(j):
        return remote(pg.at[j, 1 - g], py.at[j], p_send.at[j], p_recv.at[j], beside)

    whole = dot_rows(full[...], proj_act)
    pall = whole.reshape(experts, GROUP, rows, whole.shape[1])
    for i in range(experts):
        pg[i] = pall[i].astype(BF16)
    outer = outer[::-1] + [0]
    for j in outer:
        go(p_copy(planes[j]))

    proj_in = jnp.dot(full[...], proj_ref[...], preferred_element_type=F32)
    norm_grad = proj_in * slope * gain
    one = jnp.sum(norm_grad, axis=1, keepdims=True)
    two = jnp.sum(norm_grad * saved, axis=1, keepdims=True)
    lane = lax.broadcasted_iota(jnp.int32, (tok, 128), 1)
    packed = jnp.where(lane == 0, one, jnp.where(lane == 1, two, 0.0))
    stats[t] = packed.T[:8]

    def stat_copy(n, device, owner):
        return remote(stats.at[owner], stats.at[owner], t_send.at[n], t_recv.at[n], device)

    for n, device in ((3, across), (4, far), (5, partner)):
        go(stat_copy(n, device, t))

    def q_copy(j):
        return remote(pz_out.at[j], pz.at[j], q_send.at[j], q_recv.at[j], z_peers[j - 1])

    def join(j):
        target = planes[j]
        p_copy(target).wait_recv()
        piece = pg[target, g].astype(F32) + py[target].astype(F32)
        if j:
            pz_out[j] = piece.astype(BF16)
            go(q_copy(j))
        else:
            pgrad_ref[...] = piece

    ready = max(1, experts // 4)
    for j in outer[:ready]:
        join(j)
    for n, device in ((3, across), (4, far), (5, partner)):
        stat_copy(n, device, device[1]).wait_recv()
    total = stats[0]
    for i in range(1, tp_ways):
        total = total + stats[i]
    total = jnp.concatenate([total, jnp.zeros((120, tok), F32)], axis=0).T
    channels = saved.shape[1] * tp_ways
    mean_one = total[:, 0:1] / channels
    mean_two = total[:, 1:2] / channels
    std = jnp.broadcast_to(std_ref[...], (tok, tok)).T[:, 0:1]
    conv = std * (norm_grad - mean_one - saved * mean_two)
    ext[pl.ds(0, tok), :] = conv

    def halo_copy():
        return remote(ext.at[pl.ds(0, 32)], ext.at[pl.ds(tok, 32)], t_send.at[6], t_recv.at[6], before)

    @pl.when(s > 0)
    def _():
        halo_copy().start()

    for j in outer[ready:]:
        join(j)

    @pl.when(s < sp_ways - 1)
    def _():
        halo_copy().wait_recv()

    @pl.when(s == sp_ways - 1)
    def _():
        ext[pl.ds(tok, 32), :] = jnp.zeros((32, ext.shape[1]), F32)

    glu = taps_ref[0:1, :] * ext[pl.ds(0, tok), :]
    for k in range(1, ksize):
        glu = glu + taps_ref[k : k + 1, :] * ext[pl.ds(k, tok), :]
    in_sig = jax.nn.sigmoid(gate_ref[...].astype(F32))
    vgrad_ref[...] = (glu * in_sig).astype(BF16)
    ggrad_ref[...] = (glu * value_ref[...].astype(F32) * in_sig * (1.0 - in_sig)).astype(BF16)

    total = pgrad_ref[...]
    for j in outer[:-1]:
        q_copy(j).wait_recv()
        total = total + pz[j].astype(F32)
    pgrad_ref[...] = total

    @pl.when(s > 0)
    def _():
        halo_copy().wait_send()

    for copy in sent:
        copy.wait_send()


def mega(hidden, cot, routes, weights, w_gate, w_up, w_down, value, gate_in, normed, std, gain, taps, w_proj, experts, cap, tp_ways):
    vmem = pl.BlockSpec(memory_space=pltpu.VMEM)
    hbm = pl.BlockSpec(memory_space=pl.ANY)
    tok, width = cot.shape
    units = w_gate.shape[0]
    quarter = width // tp_ways
    padded = -(-experts // 8) * 8
    total = experts * GROUP * cap
    ch = normed.shape[1]
    rows = width // (experts * GROUP)
    half = quarter // 2
    dma = pltpu.SemaphoreType.DMA
    arrays = (hidden, cot, routes, weights, w_gate, w_up, w_down, value, gate_in, normed, std, gain, taps, w_proj)
    assert taps.shape[0] - 1 <= 32
    return pl.pallas_call(
        functools.partial(mega_kernel, experts, cap, taps.shape[0]),
        out_shape=(
            pltpu.VMEM((units, width), BF16),
            pltpu.VMEM((units, width), BF16),
            pltpu.VMEM((units, width), BF16),
            pltpu.VMEM((tok, quarter), BF16),
            pltpu.VMEM((rows, ch), F32),
            pltpu.VMEM((tok, ch), BF16),
            pltpu.VMEM((tok, ch), BF16),
        ),
        in_specs=[hbm] * len(arrays),
        out_specs=(vmem,) * 7,
        scratch_shapes=[
            pltpu.VMEM((tok, width), BF16),
            pltpu.VMEM((tok, width), BF16),
            *[pltpu.VMEM(a.shape, a.dtype) for a in (routes, weights, value, gate_in, normed, std, gain, taps, w_proj)],
            pltpu.VMEM((padded, tok), jnp.int32),
            pltpu.VMEM((padded, tok), F32),
            pltpu.VMEM((2, total, width), BF16),
            pltpu.VMEM((experts, 2, cap, quarter), BF16),
            pltpu.VMEM((units, width), BF16),
            pltpu.VMEM((units, width), BF16),
            pltpu.VMEM((units, width), BF16),
            pltpu.VMEM((total, units), BF16),
            pltpu.VMEM((total, units), BF16),
            pltpu.VMEM((total, units), BF16),
            pltpu.VMEM((units, total), BF16),
            pltpu.VMEM((total, width), BF16),
            pltpu.VMEM((experts, PAIR, GROUP * cap, quarter), BF16),
            pltpu.VMEM((2, experts, PAIR, GROUP, cap, half), BF16),
            pltpu.VMEM((experts, GROUP, cap, half), BF16),
            pltpu.VMEM((experts, PAIR, cap, half), BF16),
            pltpu.VMEM((2, experts, cap, half), BF16),
            pltpu.VMEM((2, experts, cap, half), BF16),
            pltpu.VMEM((experts, cap, quarter), BF16),
            pltpu.VMEM((experts, cap, quarter), BF16),
            pltpu.VMEM((tok, width), BF16),
            pltpu.VMEM((tp_ways, 8, tok), F32),
            pltpu.VMEM((tok + 32, ch), F32),
            pltpu.VMEM((experts, GROUP, rows, ch), BF16),
            pltpu.VMEM((experts, rows, ch), BF16),
            pltpu.VMEM((experts, rows, ch), BF16),
            pltpu.VMEM((experts, rows, ch), BF16),
            dma((4,)),
            dma((3,)),
            dma((7,)),
            dma((experts, 2, 2, 2)),
            dma((experts, 2, 2, 2)),
            dma((experts, 2, 2)),
            dma((experts, 2, 2)),
            dma((experts, PAIR)),
            dma((experts, PAIR)),
            dma((experts, 4)),
            dma((experts, 4)),
            dma((experts,)),
            dma((experts,)),
            dma((7,)),
            dma((7,)),
            dma((experts,)),
            dma((experts,)),
            dma((experts,)),
            dma((experts,)),
        ],
        compiler_params=pltpu.CompilerParams(
            collective_id=0, has_side_effects=True, vmem_limit_bytes=44 * 1024 * 1024
        ),
        name="mega",
    )(*[pltpu.with_memory_space_constraint(a, pltpu.HBM) for a in arrays])


def finish_kernel(count, *refs):
    copies = [pltpu.make_async_copy(refs[n], refs[count + n], refs[-1].at[n]) for n in range(count)]
    for copy in copies:
        copy.start()
    for copy in copies:
        copy.wait()


def finish(*arrays):
    count = len(arrays)
    return pl.pallas_call(
        functools.partial(finish_kernel, count),
        out_shape=tuple(jax.ShapeDtypeStruct(a.shape, a.dtype) for a in arrays),
        in_specs=[pl.BlockSpec(memory_space=pltpu.VMEM)] * count,
        out_specs=(pl.BlockSpec(memory_space=pl.ANY),) * count,
        scratch_shapes=[pltpu.SemaphoreType.DMA((count,))],
        compiler_params=pltpu.CompilerParams(vmem_limit_bytes=8 * 1024 * 1024),
        name="finish",
    )(*[pltpu.with_memory_space_constraint(a, pltpu.VMEM) for a in arrays])


def on_device(
    hidden_state, out_grad, routes, route_weights, w_gate, w_up, w_down,
    value, gate_in, normed, inv_std, norm_gain, taps, w_proj,
):
    tok = hidden_state.shape[0]
    top_k = routes.shape[1]
    sp_ways, tp_ways = lax.axis_size("sp"), lax.axis_size("tp")
    experts = sp_ways // GROUP
    cap = 3 * tok * top_k // (2 * experts)
    cap = -(-cap // 16) * 16
    results = mega(
        hidden_state, out_grad, routes.T, route_weights.T, w_gate[0].T, w_up[0].T, w_down[0], value, gate_in, normed,
        inv_std[None, :], norm_gain[None, :], taps, w_proj, experts, cap, tp_ways,
    )
    gate_wgrad, up_wgrad, down_grad, stream_part, proj_grad, value_grad, gate_in_grad = finish(*results)
    return gate_wgrad.T[None], up_wgrad.T[None], down_grad[None], stream_part, proj_grad, value_grad, gate_in_grad


def solution(mesh):
    in_specs = (
        P("sp", None), P("sp", None), P("sp", None), P("sp", None),
        P("sp", None, "tp"), P("sp", None, "tp"), P("sp", "tp", None),
        P("sp", "tp"), P("sp", "tp"), P("sp", "tp"), P("sp"), P("tp"), P(None, "tp"), P(None, "tp"),
    )
    out_specs = (
        P("sp", None, "tp"), P("sp", None, "tp"), P("sp", "tp", None),
        P("sp", "tp"), P("sp", "tp"), P("sp", "tp"), P("sp", "tp"),
    )
    return jax.shard_map(on_device, mesh=mesh, in_specs=in_specs, out_specs=out_specs, check_vma=False)
```

```python
import functools

import jax
import jax.numpy as jnp
from jax import lax
from jax.experimental import pallas as pl
from jax.experimental.pallas import tpu as pltpu
from jax.sharding import PartitionSpec as P

GROUP = 2
PAIR = 2
MESH = pl.DeviceIdType.MESH
F32 = jnp.float32
BF16 = jnp.bfloat16


def dot_rows(a, b):
    return lax.dot_general(a, b, (((0,), (0,)), ((), ())), preferred_element_type=F32)


def dot_cols(a, b):
    return lax.dot_general(a, b, (((1,), (1,)), ((), ())), preferred_element_type=F32)


def place():
    s, t = lax.axis_index("sp"), lax.axis_index("tp")
    e, g = s // GROUP, s % GROUP
    hi, lo = t // PAIR, t % PAIR
    across = (s, (1 - hi) * PAIR + lo)
    beside = (e * GROUP + 1 - g, t)
    partner = (s, hi * PAIR + 1 - lo)
    return s, t, e, g, hi, lo, across, beside, partner


def flip(place, bits):
    bit = 1
    while bit <= bits:
        if bits & bit:
            place = place + bit - 2 * bit * lax.rem(place // bit, 2)
        bit *= 2
    return place


def hail(devices):
    for device in devices:
        pl.semaphore_signal(pltpu.get_barrier_semaphore(), inc=1, device_id=device, device_id_type=MESH)


def greet(devices):
    pl.semaphore_wait(pltpu.get_barrier_semaphore(), len(devices))


def remote(src, dst, send, recv, device):
    return pltpu.make_async_remote_copy(
        src_ref=src, dst_ref=dst, send_sem=send, recv_sem=recv, device_id=device, device_id_type=MESH
    )


def one_hot(rank_row, cap):
    slots = lax.broadcasted_iota(jnp.int32, (cap, rank_row.shape[1]), 0)
    return jnp.where(slots == rank_row, 1.0, 0.0)


def rank_tokens(routes_ref, weights_ref, rank_ref, w_ref):
    top, tok = routes_ref.shape
    experts = lax.broadcasted_iota(jnp.int32, rank_ref.shape, 0)
    named = jnp.zeros(rank_ref.shape, F32)
    weight = jnp.zeros(rank_ref.shape, F32)
    for k in range(top):
        hit = routes_ref[k : k + 1, :] == experts
        named = jnp.where(hit, 1.0, named)
        weight = jnp.where(hit, weights_ref[k : k + 1, :], weight)
    first = lax.broadcasted_iota(jnp.int32, (tok, tok), 0)
    second = lax.broadcasted_iota(jnp.int32, (tok, tok), 1)
    earlier = jnp.where(first < second, 1.0, 0.0).astype(BF16)
    rank = jnp.dot(named.astype(BF16), earlier, preferred_element_type=F32)
    rank_ref[...] = jnp.where(named > 0.0, rank, -1.0).astype(jnp.int32)
    w_ref[...] = weight


def mega_kernel(
    experts, cap, ksize,
    h_hbm, cot_hbm, routes_hbm, weights_hbm, gate_hbm, up_hbm, down_hbm,
    value_hbm, gin_hbm, normed_hbm, std_hbm, gain_hbm, taps_hbm, proj_hbm,
    gw, uw, dw, stream_ref, pgrad_ref, vgrad_ref, ggrad_ref,
    h_ref, cot_ref, routes_ref, weights_ref, value_ref, gate_ref, normed_ref, std_ref, gain_ref, taps_ref, proj_ref,
    rank_ref, w_ref, buf, pack, wg, wu, wd, act, gg, ug, flipped, grad_ref,
    from_core, sums, rx_a, ry_b, relay, rx2, back, done, full, stats, ext, pg, py, pz_out, pz,
    h_sem, w_sem, x_sem, l_send, l_recv, c_send, c_recv,
    core_send, core_recv, hop_send, hop_recv, z_send, z_recv, t_send, t_recv, p_send, p_recv, q_send, q_recv,
):
    s, t, e, g, hi, lo, across, beside, partner = place()
    sp_ways = experts * GROUP
    tp_ways = stats.shape[0]
    tok, quarter = cot_ref.shape[0], cot_ref.shape[1] // tp_ways
    half = quarter // 2
    across_t, other_t = across[1], partner[1]
    far_t = (1 - hi) * PAIR + 1 - lo
    far = (s, far_t)
    planes = [flip(e, j) for j in range(experts)]
    z_peers = [(planes[j] * GROUP + g, t) for j in range(1, experts)]
    before = (lax.rem(s + sp_ways - 1, sp_ways), t)
    after = (lax.rem(s + 1, sp_ways), t)
    friends = z_peers + [across, beside, partner, far, before, after]
    hail(friends)
    def fetch(sem, *pairs):
        return [pltpu.make_async_copy(src, dst, sem.at[n]) for n, (src, dst) in enumerate(pairs)]

    takes = fetch(
        h_sem, (routes_hbm, routes_ref), (weights_hbm, weights_ref),
        (h_hbm, h_ref), (cot_hbm, cot_ref),
    )
    loads = fetch(w_sem, (gate_hbm, wg), (up_hbm, wu), (down_hbm, wd))
    extras = fetch(
        x_sem, (normed_hbm, normed_ref), (gain_hbm, gain_ref), (proj_hbm, proj_ref), (std_hbm, std_ref),
        (taps_hbm, taps_ref), (gin_hbm, gate_ref), (value_hbm, value_ref),
    )
    for copy in takes:
        copy.start()
    for copy in takes[:2]:
        copy.wait()
    rank_tokens(routes_ref, weights_ref, rank_ref, w_ref)
    for copy in takes[2:]:
        copy.wait()
    for copy in loads + extras:
        copy.start()
    sent = []

    def go(copy):
        copy.start()
        sent.append(copy)

    def cols_of(col):
        return pl.ds(pl.multiple_of(col * quarter, quarter), quarter)

    def rows_of(j):
        return pl.ds(pl.multiple_of(j * GROUP * cap, cap), GROUP * cap)

    def loc(j, side, col):
        return pl.ds(pl.multiple_of((j * GROUP + side) * cap, cap), cap), cols_of(col)

    def chosen(j):
        plane = pl.ds(planes[j], 1)
        hot = one_hot(rank_ref[plane, :], cap)
        return hot.astype(BF16), jnp.sum(hot * w_ref[plane, :], axis=1, keepdims=True)

    sides = (g, 1 - g)
    spread = (t, across_t)

    def spot(k, j, side, col):
        rows, cols = loc(j, sides[side], spread[col])
        return buf.at[k, rows, cols]

    def link(k, j, side, col, src, dst, device):
        return remote(src, dst, l_send.at[j, k, side, col], l_recv.at[j, k, side, col], device)

    def landed(k, j, side, col):
        ref = spot(k, j, side, col)
        link(k, j, side, col, ref, ref, partner).wait_recv()

    def pass_on(k, j, side, col, src, device):
        ref = spot(k, j, *src)
        go(link(k, j, side, col, ref, ref, device))

    def core(j, side, col):
        rows, cols = loc(j, sides[side], spread[col])
        ref = buf.at[:, rows, cols]
        return remote(ref, ref, c_send.at[j, side, col], c_recv.at[j, side, col], partner)

    def core_landed(j, side, col):
        rows, cols = loc(j, sides[side], (other_t, far_t)[col])
        ref = buf.at[:, rows, cols]
        remote(ref, ref, c_send.at[j, side, col], c_recv.at[j, side, col], partner).wait_recv()

    step = max(1, experts // 4)
    blocks = [list(range(c, min(c + step, experts))) for c in range(0, experts, step)]
    first_block, last_blocks = blocks[1], blocks[:1:-1]
    outer = [j for block in [first_block] + last_blocks + blocks[:1] for j in block if j]

    def z_out(k, j):
        return link(k, j, 0, 0, pack.at[j, k], spot(k, j, 0, 0), z_peers[j - 1])

    def z_start(block):
        for j in block:
            for k in range(2):
                z_out(k, j).start()

    later = outer[len(first_block) :]
    middle = (lax.rem(e, 4) + 1) // 2 == 1
    for j in outer:
        hot, scale = chosen(j)
        pack[j, 0] = jnp.dot(hot, h_ref[:, cols_of(t)], preferred_element_type=F32).astype(BF16)
        pack[j, 1] = (jnp.dot(hot, cot_ref[:, cols_of(t)], preferred_element_type=F32) * scale).astype(BF16)
        sent.extend(z_out(k, j) for k in range(2))
        if j == first_block[-1]:
            greet(friends)
            z_start(first_block)

    @pl.when(middle)
    def _():
        z_start(later)

    hot, scale = chosen(0)
    here = loc(0, g, t)[0]
    buf[0, here, :] = jnp.dot(hot, h_ref[...], preferred_element_type=F32).astype(BF16)
    buf[1, here, :] = (jnp.dot(hot, cot_ref[...], preferred_element_type=F32) * scale).astype(BF16)

    def d_first(j):
        for k in range(2):
            if j:
                landed(k, j, 0, 0)
                pass_on(k, j, 0, 1, (0, 0), across)
            pass_on(k, j, 1, 0, (0, 0), beside)
        if j:
            go(core(j, 0, 0))

    def d_second(j):
        if j:
            landed(0, j, 0, 1)
            pass_on(0, j, 1, 1, (0, 1), beside)
            landed(1, j, 1, 0)
            pass_on(1, j, 1, 1, (1, 0), across)
            landed(1, j, 0, 1)
            go(core(j, 0, 1))
            landed(0, j, 1, 0)
        else:
            for k in range(2):
                landed(k, j, 1, 0)
                pass_on(k, j, 1, 1, (1, 0), across)
        go(core(j, 1, 0))

    def d_third(j):
        for k in range(2):
            landed(k, j, 1, 1)
        go(core(j, 1, 1))

    def d_last(j):
        for side in range(0 if j else 1, 2):
            for col in range(2):
                core_landed(j, side, col)

    def compute(j):
        rows = rows_of(j)
        in_rows = buf[0, rows, :]
        in_cots = buf[1, rows, :]
        pre_gate = dot_cols(in_rows, wg[...])
        pre_up = dot_cols(in_rows, wu[...])
        gate_sig = jax.nn.sigmoid(pre_gate)
        silu_gate = pre_gate * gate_sig
        act_grad = dot_cols(in_cots, wd[...])
        gate_grad = (act_grad * pre_up * gate_sig * (1.0 + pre_gate * (1.0 - gate_sig))).astype(BF16)
        up_grad = (act_grad * silu_gate).astype(BF16)
        act[rows, :] = (silu_gate * pre_up).astype(BF16)
        gg[rows, :] = gate_grad
        ug[rows, :] = up_grad

    def compute_back(j):
        rows = rows_of(j)
        gate_grad, up_grad = gg[rows, :], ug[rows, :]
        for lane in (1 - lo, lo):
            for h in range(PAIR):
                cols = cols_of(h * PAIR + lane)
                grad_ref[rows, cols] = (
                    jnp.dot(gate_grad, wg[:, cols], preferred_element_type=F32)
                    + jnp.dot(up_grad, wu[:, cols], preferred_element_type=F32)
                ).astype(BF16)
                if lane is not lo and isinstance(j, int):
                    go(core_copy(j, h, 1 - lo))

    width = full.shape[1]
    piece = 256
    per_item = width // piece // 8
    units = gw.shape[0]

    def weight_item(which, n):
        if which == 0:
            if n == 0:
                flipped[pl.ds(0, units), :] = gg[...].T
                flipped[pl.ds(units, units), :] = ug[...].T

            @pl.loop(n * per_item, (n + 1) * per_item)
            def _(i):
                cols = pl.ds(pl.multiple_of(i * piece, piece), piece)
                both_grads = jnp.dot(flipped[...], buf[0, :, cols], preferred_element_type=F32).astype(BF16)
                gw[:, cols] = both_grads[:units]
                uw[:, cols] = both_grads[units:]
        else:
            if n == 0:
                flipped[pl.ds(0, units), :] = act[...].T

            @pl.loop(2 * n * per_item, 2 * (n + 1) * per_item)
            def _(i):
                cols = pl.ds(pl.multiple_of(i * piece, piece), piece)
                dw[:, cols] = jnp.dot(
                    flipped[pl.ds(0, units), :], buf[1, :, cols], preferred_element_type=F32
                ).astype(BF16)

    items = [(0, n) for n in range(8)] + [(1, n) for n in range(4)]

    def fill(count=1):
        for _ in range(count):
            if items:
                weight_item(*items.pop(0))

    def core_copy(j, h, lane):
        return remote(
            grad_ref.at[rows_of(j), cols_of(h * PAIR + lane)],
            from_core.at[j, h], core_send.at[j, h], core_recv.at[j, h], partner,
        )

    def hop_copy(n, j, src, dst, device):
        return remote(src, dst, hop_send.at[j, n], hop_recv.at[j, n], device)

    def x_first(j):
        return hop_copy(0, j, sums.at[0, j, 1 - hi], rx_a.at[j], across)

    def y_first(j):
        return hop_copy(1, j, sums.at[1, j, :, 1 - g], ry_b.at[j], beside)

    def y_second(j):
        return hop_copy(2, j, relay.at[0, j], rx2.at[0, j], beside)

    def x_second(j):
        return hop_copy(3, j, relay.at[1, j], rx2.at[1, j], across)

    def z_copy(j):
        return remote(done.at[j], back.at[j], z_send.at[j], z_recv.at[j], z_peers[j - 1])

    def first(j):
        for h in range(PAIR):
            core_copy(j, h, lo).wait_recv()
            mine = grad_ref[rows_of(j), cols_of(h * PAIR + lo)].astype(F32)
            total = (mine + from_core[j, h].astype(F32)).astype(BF16).reshape(GROUP, cap, quarter)
            sums[0, j, h] = total[:, :, :half]
            sums[1, j, h] = total[:, :, half:]
        go(x_first(j))
        go(y_first(j))

    def second(j):
        x_first(j).wait_recv()
        relay[0, j] = (sums[0, j, hi, 1 - g].astype(F32) + rx_a[j, 1 - g].astype(F32)).astype(BF16)
        go(y_second(j))
        y_first(j).wait_recv()
        relay[1, j] = (sums[1, j, 1 - hi, g].astype(F32) + ry_b[j, 1 - hi].astype(F32)).astype(BF16)
        go(x_second(j))

    def third(j):
        y_second(j).wait_recv()
        done[j, :, :half] = (
            sums[0, j, hi, g].astype(F32) + rx_a[j, g].astype(F32) + rx2[0, j].astype(F32)
        ).astype(BF16)
        x_second(j).wait_recv()
        done[j, :, half:] = (
            sums[1, j, hi, g].astype(F32) + ry_b[j, hi].astype(F32) + rx2[1, j].astype(F32)
        ).astype(BF16)
        if j:
            go(z_copy(j))

    def flow(*stages):
        for stage, block in stages:
            for j in block:
                stage(j)

    def work(block, *stages):
        for stage in stages:
            if len(block) == 1:
                stage(block[0])
            else:
                pl.loop(block[0], block[-1] + 1)(stage)
        if len(block) > 1 and compute_back in stages:
            for j in block:
                for h in range(PAIR):
                    go(core_copy(j, h, 1 - lo))

    own, near, far_one, far_two = blocks[0], first_block, *last_blocks
    d_first(0)
    flow((d_first, near))

    @pl.when(jnp.logical_not(middle))
    def _():
        z_start(later)

    flow((d_first, own[1:]), (d_second, own), (d_second, near), (d_first, far_one), (d_third, near))
    flow((d_last, near), (d_first, far_two))
    for copy in loads:
        copy.wait()
    work(near, compute, compute_back)
    flow((d_second, far_one), (d_third, own), (d_last, own))
    work(own, compute)
    flow((d_second, far_two), (first, near), (d_third, far_one), (d_last, far_one))
    work(far_one, compute, compute_back)
    flow((d_third, far_two), (first, far_one), (d_last, far_two), (second, near))
    work(far_two, compute, compute_back)
    flow((first, far_two))
    work(own, compute_back)
    flow((second, far_one), (third, near))
    fill(2)
    flow((second, far_two), (first, own))
    fill(1)
    flow((third, far_one))
    fill(1)
    flow((third, far_two))
    fill(1)
    flow((second, own))
    fill(2)
    flow((third, own))
    fill(1)

    for copy in extras:
        copy.wait()
    gain = gain_ref[...]
    saved = normed_ref[...].astype(F32)
    pre_act = saved * gain
    act_sig = jax.nn.sigmoid(pre_act)
    slope = act_sig * (1.0 + pre_act * (1.0 - act_sig))
    proj_act = (pre_act * act_sig).astype(BF16)

    stream = cot_ref[:, cols_of(t)].astype(F32)
    for j in [0] + [k for block in (near, far_one, far_two, own[1:]) for k in block]:
        if j:
            z_copy(j).wait_recv()
            block = back[j]
        else:
            block = done[0]
        hot = one_hot(rank_ref[pl.ds(planes[j], 1), :], cap).astype(BF16)
        stream = stream + dot_rows(hot, block)
    stream = stream.astype(BF16)
    stream_ref[...] = stream
    full[:, cols_of(t)] = stream

    def gather_copy(n, col, device):
        return remote(full.at[:, cols_of(col)], full.at[:, cols_of(col)], t_send.at[n], t_recv.at[n], device)

    rows = pg.shape[2]
    share = experts // tp_ways

    def p_copy(plane):
        return remote(pg.at[plane, 1 - g], py.at[plane], p_send.at[plane], p_recv.at[plane], beside)

    def q_copy(plane):
        return remote(pz_out.at[plane], pz.at[e], q_send.at[plane], q_recv.at[e], (plane * GROUP + g, t))

    def part(col):
        block = full[:, cols_of(col)]
        pall = dot_rows(block, proj_act).reshape(share, GROUP, rows, proj_act.shape[1]).astype(BF16)
        for n in range(share):
            pg[col * share + n] = pall[n]
        for n in range(share):
            go(p_copy(col * share + n))
        taken = proj_ref[pl.ds(pl.multiple_of(col * quarter, quarter), quarter), :]
        return jnp.dot(block, taken, preferred_element_type=F32)

    def join(col):
        for n in range(share):
            plane = col * share + n
            p_copy(plane).wait_recv()
            piece = pg[plane, g].astype(F32) + py[plane].astype(F32)
            pz_out[plane] = piece.astype(BF16)

            @pl.when(plane == e)
            def _():
                pgrad_ref[...] = piece

            @pl.when(plane != e)
            def _():
                q_copy(plane).start()

    go(gather_copy(0, t, across))
    go(gather_copy(1, t, partner))
    proj_in = part(t)
    gather_copy(1, other_t, partner).wait_recv()
    proj_in = proj_in + part(other_t)
    fill(1)
    join(t)
    gather_copy(0, across_t, across).wait_recv()
    go(gather_copy(2, across_t, partner))
    proj_in = proj_in + part(across_t)
    join(other_t)
    gather_copy(2, far_t, partner).wait_recv()
    proj_in = proj_in + part(far_t)
    norm_grad = proj_in * slope * gain
    one = jnp.sum(norm_grad, axis=1, keepdims=True)
    two = jnp.sum(norm_grad * saved, axis=1, keepdims=True)
    lane = lax.broadcasted_iota(jnp.int32, (tok, 128), 1)
    packed = jnp.where(lane == 0, one, jnp.where(lane == 1, two, 0.0))
    stats[t] = packed.T[:8]

    def stat_copy(n, device, owner):
        return remote(stats.at[owner], stats.at[owner], t_send.at[n], t_recv.at[n], device)

    for n, device in ((3, across), (4, far), (5, partner)):
        go(stat_copy(n, device, t))
    fill(1)
    join(across_t)
    for n, device in ((3, across), (4, far), (5, partner)):
        stat_copy(n, device, device[1]).wait_recv()
    total = stats[0]
    for i in range(1, tp_ways):
        total = total + stats[i]
    total = jnp.concatenate([total, jnp.zeros((120, tok), F32)], axis=0).T
    channels = saved.shape[1] * tp_ways
    mean_one = total[:, 0:1] / channels
    mean_two = total[:, 1:2] / channels
    std = jnp.broadcast_to(std_ref[...], (tok, tok)).T[:, 0:1]
    conv = std * (norm_grad - mean_one - saved * mean_two)
    ext[pl.ds(0, tok), :] = conv

    def halo_copy():
        return remote(ext.at[pl.ds(0, 32)], ext.at[pl.ds(tok, 32)], t_send.at[6], t_recv.at[6], before)

    @pl.when(s > 0)
    def _():
        halo_copy().start()

    join(far_t)
    fill(len(items))

    @pl.when(s < sp_ways - 1)
    def _():
        halo_copy().wait_recv()

    @pl.when(s == sp_ways - 1)
    def _():
        ext[pl.ds(tok, 32), :] = jnp.zeros((32, ext.shape[1]), F32)

    glu = taps_ref[0:1, :] * ext[pl.ds(0, tok), :]
    for k in range(1, ksize):
        glu = glu + taps_ref[k : k + 1, :] * ext[pl.ds(k, tok), :]
    in_sig = jax.nn.sigmoid(gate_ref[...].astype(F32))
    vgrad_ref[...] = (glu * in_sig).astype(BF16)
    ggrad_ref[...] = (glu * value_ref[...].astype(F32) * in_sig * (1.0 - in_sig)).astype(BF16)

    def q_arrival(j):
        plane = planes[j]
        return remote(pz_out.at[plane], pz.at[plane], q_send.at[plane], q_recv.at[plane], z_peers[j - 1])

    total = pgrad_ref[...]
    for j in range(1, experts):
        q_arrival(j).wait_recv()
        total = total + pz[planes[j]].astype(F32)
    pgrad_ref[...] = total

    @pl.when(s > 0)
    def _():
        halo_copy().wait_send()

    for copy in sent + [q_arrival(j) for j in range(1, experts)]:
        copy.wait_send()


def mega(hidden, cot, routes, weights, w_gate, w_up, w_down, value, gate_in, normed, std, gain, taps, w_proj, experts, cap, tp_ways):
    vmem = pl.BlockSpec(memory_space=pltpu.VMEM)
    hbm = pl.BlockSpec(memory_space=pl.ANY)
    tok, width = cot.shape
    units = w_gate.shape[0]
    quarter = width // tp_ways
    padded = -(-experts // 8) * 8
    total = experts * GROUP * cap
    ch = normed.shape[1]
    rows = width // (experts * GROUP)
    half = quarter // 2
    dma = pltpu.SemaphoreType.DMA
    arrays = (hidden, cot, routes, weights, w_gate, w_up, w_down, value, gate_in, normed, std, gain, taps, w_proj)
    assert taps.shape[0] - 1 <= 32
    return pl.pallas_call(
        functools.partial(mega_kernel, experts, cap, taps.shape[0]),
        out_shape=(
            pltpu.VMEM((units, width), BF16),
            pltpu.VMEM((units, width), BF16),
            pltpu.VMEM((units, width), BF16),
            pltpu.VMEM((tok, quarter), BF16),
            pltpu.VMEM((rows, ch), F32),
            pltpu.VMEM((tok, ch), BF16),
            pltpu.VMEM((tok, ch), BF16),
        ),
        in_specs=[hbm] * len(arrays),
        out_specs=(vmem,) * 7,
        scratch_shapes=[
            pltpu.VMEM((tok, width), BF16),
            pltpu.VMEM((tok, width), BF16),
            *[pltpu.VMEM(a.shape, a.dtype) for a in (routes, weights, value, gate_in, normed, std, gain, taps, w_proj)],
            pltpu.VMEM((padded, tok), jnp.int32),
            pltpu.VMEM((padded, tok), F32),
            pltpu.VMEM((2, total, width), BF16),
            pltpu.VMEM((experts, 2, cap, quarter), BF16),
            pltpu.VMEM((units, width), BF16),
            pltpu.VMEM((units, width), BF16),
            pltpu.VMEM((units, width), BF16),
            pltpu.VMEM((total, units), BF16),
            pltpu.VMEM((total, units), BF16),
            pltpu.VMEM((total, units), BF16),
            pltpu.VMEM((2 * units, total), BF16),
            pltpu.VMEM((total, width), BF16),
            pltpu.VMEM((experts, PAIR, GROUP * cap, quarter), BF16),
            pltpu.VMEM((2, experts, PAIR, GROUP, cap, half), BF16),
            pltpu.VMEM((experts, GROUP, cap, half), BF16),
            pltpu.VMEM((experts, PAIR, cap, half), BF16),
            pltpu.VMEM((2, experts, cap, half), BF16),
            pltpu.VMEM((2, experts, cap, half), BF16),
            pltpu.VMEM((experts, cap, quarter), BF16),
            pltpu.VMEM((experts, cap, quarter), BF16),
            pltpu.VMEM((tok, width), BF16),
            pltpu.VMEM((tp_ways, 8, tok), F32),
            pltpu.VMEM((tok + 32, ch), F32),
            pltpu.VMEM((experts, GROUP, rows, ch), BF16),
            pltpu.VMEM((experts, rows, ch), BF16),
            pltpu.VMEM((experts, rows, ch), BF16),
            pltpu.VMEM((experts, rows, ch), BF16),
            dma((4,)),
            dma((3,)),
            dma((7,)),
            dma((experts, 2, 2, 2)),
            dma((experts, 2, 2, 2)),
            dma((experts, 2, 2)),
            dma((experts, 2, 2)),
            dma((experts, PAIR)),
            dma((experts, PAIR)),
            dma((experts, 4)),
            dma((experts, 4)),
            dma((experts,)),
            dma((experts,)),
            dma((7,)),
            dma((7,)),
            dma((experts,)),
            dma((experts,)),
            dma((experts,)),
            dma((experts,)),
        ],
        compiler_params=pltpu.CompilerParams(
            collective_id=0, has_side_effects=True, vmem_limit_bytes=44 * 1024 * 1024
        ),
        name="mega",
    )(*[pltpu.with_memory_space_constraint(a, pltpu.HBM) for a in arrays])


def finish_kernel(count, *refs):
    copies = [pltpu.make_async_copy(refs[n], refs[count + n], refs[-1].at[n]) for n in range(count)]
    for copy in copies:
        copy.start()
    for copy in copies:
        copy.wait()


def finish(*arrays):
    count = len(arrays)
    return pl.pallas_call(
        functools.partial(finish_kernel, count),
        out_shape=tuple(jax.ShapeDtypeStruct(a.shape, a.dtype) for a in arrays),
        in_specs=[pl.BlockSpec(memory_space=pltpu.VMEM)] * count,
        out_specs=(pl.BlockSpec(memory_space=pl.ANY),) * count,
        scratch_shapes=[pltpu.SemaphoreType.DMA((count,))],
        compiler_params=pltpu.CompilerParams(vmem_limit_bytes=8 * 1024 * 1024),
        name="finish",
    )(*[pltpu.with_memory_space_constraint(a, pltpu.VMEM) for a in arrays])


def on_device(
    hidden_state, out_grad, routes, route_weights, w_gate, w_up, w_down,
    value, gate_in, normed, inv_std, norm_gain, taps, w_proj,
):
    tok = hidden_state.shape[0]
    top_k = routes.shape[1]
    sp_ways, tp_ways = lax.axis_size("sp"), lax.axis_size("tp")
    experts = sp_ways // GROUP
    cap = 3 * tok * top_k // (2 * experts)
    cap = -(-cap // 16) * 16
    results = mega(
        hidden_state, out_grad, routes.T, route_weights.T, w_gate[0].T, w_up[0].T, w_down[0], value, gate_in, normed,
        inv_std[None, :], norm_gain[None, :], taps, w_proj, experts, cap, tp_ways,
    )
    gate_wgrad, up_wgrad, down_grad, stream_part, proj_grad, value_grad, gate_in_grad = finish(*results)
    return gate_wgrad.T[None], up_wgrad.T[None], down_grad[None], stream_part, proj_grad, value_grad, gate_in_grad


def solution(mesh):
    in_specs = (
        P("sp", None), P("sp", None), P("sp", None), P("sp", None),
        P("sp", None, "tp"), P("sp", None, "tp"), P("sp", "tp", None),
        P("sp", "tp"), P("sp", "tp"), P("sp", "tp"), P("sp"), P("tp"), P(None, "tp"), P(None, "tp"),
    )
    out_specs = (
        P("sp", None, "tp"), P("sp", None, "tp"), P("sp", "tp", None),
        P("sp", "tp"), P("sp", "tp"), P("sp", "tp"), P("sp", "tp"),
    )
    return jax.shard_map(on_device, mesh=mesh, in_specs=in_specs, out_specs=out_specs, check_vma=False)
```

```python
import functools

import jax
import jax.numpy as jnp
from jax import lax
from jax.experimental import pallas as pl
from jax.experimental.pallas import tpu as pltpu
from jax.sharding import PartitionSpec as P

GROUP = 2
PAIR = 2
MESH = pl.DeviceIdType.MESH
F32 = jnp.float32
BF16 = jnp.bfloat16


def dot_rows(a, b):
    return lax.dot_general(a, b, (((0,), (0,)), ((), ())), preferred_element_type=F32)


def dot_cols(a, b):
    return lax.dot_general(a, b, (((1,), (1,)), ((), ())), preferred_element_type=F32)


def place():
    s, t = lax.axis_index("sp"), lax.axis_index("tp")
    e, g = s // GROUP, s % GROUP
    hi, lo = t // PAIR, t % PAIR
    across = (s, (1 - hi) * PAIR + lo)
    beside = (e * GROUP + 1 - g, t)
    partner = (s, hi * PAIR + 1 - lo)
    return s, t, e, g, hi, lo, across, beside, partner


def flip(place, bits):
    bit = 1
    while bit <= bits:
        if bits & bit:
            place = place + bit - 2 * bit * lax.rem(place // bit, 2)
        bit *= 2
    return place


def hail(devices):
    for device in devices:
        pl.semaphore_signal(pltpu.get_barrier_semaphore(), inc=1, device_id=device, device_id_type=MESH)


def greet(devices):
    pl.semaphore_wait(pltpu.get_barrier_semaphore(), len(devices))


def remote(src, dst, send, recv, device):
    return pltpu.make_async_remote_copy(
        src_ref=src, dst_ref=dst, send_sem=send, recv_sem=recv, device_id=device, device_id_type=MESH
    )


def one_hot(rank_row, cap):
    slots = lax.broadcasted_iota(jnp.int32, (cap, rank_row.shape[1]), 0)
    return jnp.where(slots == rank_row, 1.0, 0.0)


def rank_tokens(routes_ref, weights_ref, rank_ref, w_ref):
    top, tok = routes_ref.shape
    experts = lax.broadcasted_iota(jnp.int32, rank_ref.shape, 0)
    named = jnp.zeros(rank_ref.shape, F32)
    weight = jnp.zeros(rank_ref.shape, F32)
    for k in range(top):
        hit = routes_ref[k : k + 1, :] == experts
        named = jnp.where(hit, 1.0, named)
        weight = jnp.where(hit, weights_ref[k : k + 1, :], weight)
    first = lax.broadcasted_iota(jnp.int32, (tok, tok), 0)
    second = lax.broadcasted_iota(jnp.int32, (tok, tok), 1)
    earlier = jnp.where(first < second, 1.0, 0.0).astype(BF16)
    rank = jnp.dot(named.astype(BF16), earlier, preferred_element_type=F32)
    rank_ref[...] = jnp.where(named > 0.0, rank, -1.0).astype(jnp.int32)
    w_ref[...] = weight


def mega_kernel(
    experts, cap, ksize,
    h_hbm, cot_hbm, routes_hbm, weights_hbm, gate_hbm, up_hbm, down_hbm,
    value_hbm, gin_hbm, normed_hbm, std_hbm, gain_hbm, taps_hbm, proj_hbm,
    gw, uw, dw, stream_ref, pgrad_ref, vgrad_ref, ggrad_ref,
    h_ref, cot_ref, routes_ref, weights_ref, value_ref, gate_ref, normed_ref, std_ref, gain_ref, taps_ref, proj_ref,
    rank_ref, w_ref, buf, pack, wg, wu, wd, act, gg, ug, flipped, grad_ref,
    from_core, sums, rx_a, ry_b, relay, rx2, back, done, full, stats, ext, pg, py, pz_out, pz,
    h_sem, w_sem, x_sem, l_send, l_recv, c_send, c_recv,
    core_send, core_recv, hop_send, hop_recv, z_send, z_recv, t_send, t_recv, p_send, p_recv, q_send, q_recv,
):
    s, t, e, g, hi, lo, across, beside, partner = place()
    sp_ways = experts * GROUP
    tp_ways = stats.shape[0]
    tok, quarter = cot_ref.shape[0], cot_ref.shape[1] // tp_ways
    half = quarter // 2
    across_t, other_t = across[1], partner[1]
    far_t = (1 - hi) * PAIR + 1 - lo
    far = (s, far_t)
    planes = [flip(e, j) for j in range(experts)]
    z_peers = [(planes[j] * GROUP + g, t) for j in range(1, experts)]
    before = (lax.rem(s + sp_ways - 1, sp_ways), t)
    after = (lax.rem(s + 1, sp_ways), t)
    friends = z_peers + [across, beside, partner, far, before, after]
    hail(friends)
    def fetch(sem, *pairs):
        return [pltpu.make_async_copy(src, dst, sem.at[n]) for n, (src, dst) in enumerate(pairs)]

    takes = fetch(
        h_sem, (routes_hbm, routes_ref), (weights_hbm, weights_ref),
        (h_hbm, h_ref), (cot_hbm, cot_ref),
    )
    loads = fetch(w_sem, (gate_hbm, wg), (up_hbm, wu), (down_hbm, wd))
    extras = fetch(
        x_sem, (normed_hbm, normed_ref), (gain_hbm, gain_ref), (proj_hbm, proj_ref), (std_hbm, std_ref),
        (taps_hbm, taps_ref), (gin_hbm, gate_ref), (value_hbm, value_ref),
    )
    for copy in takes:
        copy.start()
    for copy in takes[:2]:
        copy.wait()
    rank_tokens(routes_ref, weights_ref, rank_ref, w_ref)
    for copy in takes[2:]:
        copy.wait()
    for copy in loads + extras:
        copy.start()
    sent = []

    def go(copy):
        copy.start()
        sent.append(copy)

    def cols_of(col):
        return pl.ds(pl.multiple_of(col * quarter, quarter), quarter)

    def rows_of(j):
        return pl.ds(pl.multiple_of(j * GROUP * cap, cap), GROUP * cap)

    def loc(j, side, col):
        return pl.ds(pl.multiple_of((j * GROUP + side) * cap, cap), cap), cols_of(col)

    def chosen(j):
        plane = pl.ds(planes[j], 1)
        hot = one_hot(rank_ref[plane, :], cap)
        return hot.astype(BF16), jnp.sum(hot * w_ref[plane, :], axis=1, keepdims=True)

    sides = (g, 1 - g)
    spread = (t, across_t)

    def spot(k, j, side, col):
        rows, cols = loc(j, sides[side], spread[col])
        return buf.at[k, rows, cols]

    def link(k, j, side, col, src, dst, device):
        return remote(src, dst, l_send.at[j, k, side, col], l_recv.at[j, k, side, col], device)

    def landed(k, j, side, col):
        ref = spot(k, j, side, col)
        link(k, j, side, col, ref, ref, partner).wait_recv()

    def pass_on(k, j, side, col, src, device):
        ref = spot(k, j, *src)
        go(link(k, j, side, col, ref, ref, device))

    def core(j, side, col):
        rows, cols = loc(j, sides[side], spread[col])
        ref = buf.at[:, rows, cols]
        return remote(ref, ref, c_send.at[j, side, col], c_recv.at[j, side, col], partner)

    def core_landed(j, side, col):
        rows, cols = loc(j, sides[side], (other_t, far_t)[col])
        ref = buf.at[:, rows, cols]
        remote(ref, ref, c_send.at[j, side, col], c_recv.at[j, side, col], partner).wait_recv()

    step = max(1, experts // 4)
    blocks = [list(range(c, min(c + step, experts))) for c in range(0, experts, step)]
    first_block, last_blocks = blocks[1], blocks[:1:-1]
    outer = [j for block in [first_block] + last_blocks + blocks[:1] for j in block if j]

    def z_out(k, j):
        return link(k, j, 0, 0, pack.at[j, k], spot(k, j, 0, 0), z_peers[j - 1])

    def z_start(block):
        for j in block:
            for k in range(2):
                z_out(k, j).start()

    far_one, far_two = last_blocks
    rest = blocks[0][1:]
    middle = (lax.rem(e, 4) + 1) // 2 == 1
    for j in outer:
        hot, scale = chosen(j)
        pack[j, 0] = jnp.dot(hot, h_ref[:, cols_of(t)], preferred_element_type=F32).astype(BF16)
        pack[j, 1] = (jnp.dot(hot, cot_ref[:, cols_of(t)], preferred_element_type=F32) * scale).astype(BF16)
        sent.extend(z_out(k, j) for k in range(2))
        if j == first_block[-1]:
            greet(friends)
            z_start(first_block)

    @pl.when(middle)
    def _():
        z_start(far_one)

    hot, scale = chosen(0)
    here = loc(0, g, t)[0]
    buf[0, here, :] = jnp.dot(hot, h_ref[...], preferred_element_type=F32).astype(BF16)
    buf[1, here, :] = (jnp.dot(hot, cot_ref[...], preferred_element_type=F32) * scale).astype(BF16)

    def d_first(j):
        for k in range(2):
            if j:
                landed(k, j, 0, 0)
                pass_on(k, j, 0, 1, (0, 0), across)
            pass_on(k, j, 1, 0, (0, 0), beside)
        if j:
            go(core(j, 0, 0))

    def d_second(j):
        if j:
            landed(0, j, 0, 1)
            pass_on(0, j, 1, 1, (0, 1), beside)
            landed(1, j, 1, 0)
            pass_on(1, j, 1, 1, (1, 0), across)
            landed(1, j, 0, 1)
            go(core(j, 0, 1))
            landed(0, j, 1, 0)
        else:
            for k in range(2):
                landed(k, j, 1, 0)
                pass_on(k, j, 1, 1, (1, 0), across)
        go(core(j, 1, 0))

    def d_third(j):
        for k in range(2):
            landed(k, j, 1, 1)
        go(core(j, 1, 1))

    def d_last(j):
        for side in range(0 if j else 1, 2):
            for col in range(2):
                core_landed(j, side, col)

    def compute(j):
        rows = rows_of(j)
        in_rows = buf[0, rows, :]
        in_cots = buf[1, rows, :]
        pre_gate = dot_cols(in_rows, wg[...])
        pre_up = dot_cols(in_rows, wu[...])
        gate_sig = jax.nn.sigmoid(pre_gate)
        silu_gate = pre_gate * gate_sig
        act_grad = dot_cols(in_cots, wd[...])
        gate_grad = (act_grad * pre_up * gate_sig * (1.0 + pre_gate * (1.0 - gate_sig))).astype(BF16)
        up_grad = (act_grad * silu_gate).astype(BF16)
        act[rows, :] = (silu_gate * pre_up).astype(BF16)
        gg[rows, :] = gate_grad
        ug[rows, :] = up_grad

    def compute_back(j):
        rows = rows_of(j)
        gate_grad, up_grad = gg[rows, :], ug[rows, :]
        for lane in (1 - lo, lo):
            for h in range(PAIR):
                cols = cols_of(lane * PAIR + h)
                grad_ref[rows, cols] = (
                    jnp.dot(gate_grad, wg[:, cols], preferred_element_type=F32)
                    + jnp.dot(up_grad, wu[:, cols], preferred_element_type=F32)
                ).astype(BF16)
                if lane is not lo and isinstance(j, int):
                    go(core_copy(j, h, 1 - lo))

    width = full.shape[1]
    piece = 256
    per_item = width // piece // 8
    units = gw.shape[0]

    def weight_item(which, n):
        if which == 0:
            if n == 0:
                flipped[pl.ds(0, units), :] = gg[...].T
                flipped[pl.ds(units, units), :] = ug[...].T

            @pl.loop(n * per_item, (n + 1) * per_item)
            def _(i):
                cols = pl.ds(pl.multiple_of(i * piece, piece), piece)
                both_grads = jnp.dot(flipped[...], buf[0, :, cols], preferred_element_type=F32).astype(BF16)
                gw[:, cols] = both_grads[:units]
                uw[:, cols] = both_grads[units:]
        else:
            if n == 0:
                flipped[pl.ds(0, units), :] = act[...].T

            @pl.loop(2 * n * per_item, 2 * (n + 1) * per_item)
            def _(i):
                cols = pl.ds(pl.multiple_of(i * piece, piece), piece)
                dw[:, cols] = jnp.dot(
                    flipped[pl.ds(0, units), :], buf[1, :, cols], preferred_element_type=F32
                ).astype(BF16)

    items = [(0, n) for n in range(8)] + [(1, n) for n in range(4)]

    def fill(count=1):
        for _ in range(count):
            if items:
                weight_item(*items.pop(0))

    def core_copy(j, h, lane):
        return remote(
            grad_ref.at[rows_of(j), cols_of(lane * PAIR + h)],
            from_core.at[j, h], core_send.at[j, h], core_recv.at[j, h], partner,
        )

    def hop_copy(n, j, src, dst, device):
        return remote(src, dst, hop_send.at[j, n], hop_recv.at[j, n], device)

    def x_first(j):
        return hop_copy(0, j, sums.at[0, j, 1 - hi], rx_a.at[j], across)

    def y_first(j):
        return hop_copy(1, j, sums.at[1, j, :, 1 - g], ry_b.at[j], beside)

    def y_second(j):
        return hop_copy(2, j, relay.at[0, j], rx2.at[0, j], beside)

    def x_second(j):
        return hop_copy(3, j, relay.at[1, j], rx2.at[1, j], across)

    def z_copy(j):
        return remote(done.at[j], back.at[j], z_send.at[j], z_recv.at[j], z_peers[j - 1])

    def first(j):
        for h in range(PAIR):
            core_copy(j, h, lo).wait_recv()
            mine = grad_ref[rows_of(j), cols_of(lo * PAIR + h)].astype(F32)
            total = (mine + from_core[j, h].astype(F32)).astype(BF16).reshape(GROUP, cap, quarter)
            sums[0, j, h] = total[:, :, :half]
            sums[1, j, h] = total[:, :, half:]
        go(x_first(j))
        go(y_first(j))

    def second(j):
        x_first(j).wait_recv()
        relay[0, j] = (sums[0, j, hi, 1 - g].astype(F32) + rx_a[j, 1 - g].astype(F32)).astype(BF16)
        go(y_second(j))
        y_first(j).wait_recv()
        relay[1, j] = (sums[1, j, 1 - hi, g].astype(F32) + ry_b[j, 1 - hi].astype(F32)).astype(BF16)
        go(x_second(j))

    def third(j):
        y_second(j).wait_recv()
        done[j, :, :half] = (
            sums[0, j, hi, g].astype(F32) + rx_a[j, g].astype(F32) + rx2[0, j].astype(F32)
        ).astype(BF16)
        x_second(j).wait_recv()
        done[j, :, half:] = (
            sums[1, j, hi, g].astype(F32) + ry_b[j, hi].astype(F32) + rx2[1, j].astype(F32)
        ).astype(BF16)
        if j:
            go(z_copy(j))

    def flow(*stages):
        for stage, block in stages:
            for j in block:
                stage(j)

    def work(block, *stages):
        for stage in stages:
            if len(block) == 1:
                stage(block[0])
            else:
                pl.loop(block[0], block[-1] + 1)(stage)
        if len(block) > 1 and compute_back in stages:
            for j in block:
                for h in range(PAIR):
                    go(core_copy(j, h, 1 - lo))

    own, near = blocks[0], first_block
    d_first(0)
    flow((d_first, near))

    @pl.when(middle)
    def _():
        z_start(far_two + rest)

    flow((d_second, [0]))

    @pl.when(jnp.logical_not(middle))
    def _():
        z_start(far_one)

    flow((d_second, near), (d_first, far_one))

    @pl.when(jnp.logical_not(middle))
    def _():
        z_start(far_two + rest)

    flow((d_third, near))
    flow((d_last, near), (d_first, far_two))
    for copy in loads:
        copy.wait()
    work(near, compute, compute_back)
    flow((d_second, far_one), (d_first, rest), (d_second, rest), (d_third, own), (d_last, own))
    work(own, compute)
    flow((d_second, far_two), (first, near))
    work(own, compute_back)
    flow((d_third, far_one), (d_last, far_one), (first, own))
    work(far_one, compute, compute_back)
    flow((d_third, far_two), (first, far_one), (d_last, far_two), (second, near), (second, own))
    work(far_two, compute, compute_back)
    flow((second, far_one), (first, far_two), (third, near), (third, own))
    fill(2)
    flow((third, far_one))
    fill(2)
    flow((second, far_two))
    fill(2)
    flow((third, far_two))
    fill(5)

    for copy in extras:
        copy.wait()
    gain = gain_ref[...]
    saved = normed_ref[...].astype(F32)
    pre_act = saved * gain
    act_sig = jax.nn.sigmoid(pre_act)
    slope = act_sig * (1.0 + pre_act * (1.0 - act_sig))
    proj_act = (pre_act * act_sig).astype(BF16)

    own_q, other_q = lo * PAIR + hi, (1 - lo) * PAIR + hi
    across_q, far_q = lo * PAIR + 1 - hi, (1 - lo) * PAIR + 1 - hi
    stream = cot_ref[:, cols_of(own_q)].astype(F32)
    for j in [0] + [k for block in (near, far_one, far_two, own[1:]) for k in block]:
        if j:
            z_copy(j).wait_recv()
            block = back[j]
        else:
            block = done[0]
        hot = one_hot(rank_ref[pl.ds(planes[j], 1), :], cap).astype(BF16)
        stream = stream + dot_rows(hot, block)
    full[:, cols_of(own_q)] = stream.astype(BF16)

    def strip(col, n):
        return pl.ds(pl.multiple_of(col * quarter + seq[n] * half, half), half)

    def gather_copy(n, k, col, device):
        ref = full.at[:, strip(col, n)]
        return remote(ref, ref, t_send.at[2 * k + n], t_recv.at[2 * k + n], device)

    rows = pg.shape[2]
    share = experts // tp_ways
    seq = (1 - g, g) if share == 1 else (0, 1)

    def p_copy(plane):
        return remote(pg.at[plane, 1 - g], py.at[plane], p_send.at[plane], p_recv.at[plane], beside)

    def q_copy(plane):
        return remote(pz_out.at[plane], pz.at[e], q_send.at[plane], q_recv.at[e], (plane * GROUP + g, t))

    def part(col, n):
        block = full[:, strip(col, n)]
        pall = dot_rows(block, proj_act).astype(BF16)
        if share == 1:
            pg[col, seq[n]] = pall
            planes_here = [col] * (1 - n)
        else:
            pall = pall.reshape(share // 2, GROUP, rows, proj_act.shape[1])
            planes_here = [col * share + n * (share // 2) + m for m in range(share // 2)]
            for m, plane in enumerate(planes_here):
                pg[plane] = pall[m]
        for plane in planes_here:
            go(p_copy(plane))
        return jnp.dot(block, proj_ref[strip(col, n), :], preferred_element_type=F32)

    def join(col):
        for n in range(share):
            plane = col * share + n
            p_copy(plane).wait_recv()
            piece = pg[plane, g].astype(F32) + py[plane].astype(F32)
            pz_out[plane] = piece.astype(BF16)

            @pl.when(plane == e)
            def _():
                pgrad_ref[...] = piece

            @pl.when(plane != e)
            def _():
                q_copy(plane).start()

    for n in range(2):
        go(gather_copy(n, 0, own_q, across))
        go(gather_copy(n, 1, own_q, partner))
    proj_in = part(own_q, 0) + part(own_q, 1)
    for n in range(2):
        gather_copy(n, 1, other_q, partner).wait_recv()
        proj_in = proj_in + part(other_q, n)
    for n in range(2):
        gather_copy(n, 0, across_q, across).wait_recv()
        go(gather_copy(n, 2, across_q, partner))
        proj_in = proj_in + part(across_q, n)
        join((own_q, other_q)[n])
        gather_copy(n, 2, far_q, partner).wait_recv()
        proj_in = proj_in + part(far_q, n)
    stream_ref[...] = full[:, cols_of(t)]
    norm_grad = proj_in * slope * gain
    one = jnp.sum(norm_grad, axis=1, keepdims=True)
    two = jnp.sum(norm_grad * saved, axis=1, keepdims=True)
    lane = lax.broadcasted_iota(jnp.int32, (tok, 128), 1)
    packed = jnp.where(lane == 0, one, jnp.where(lane == 1, two, 0.0))
    stats[t] = packed.T[:8]

    def stat_copy(n, device, owner):
        return remote(stats.at[owner], stats.at[owner], t_send.at[n], t_recv.at[n], device)

    for n, device in ((6, across), (7, far), (8, partner)):
        go(stat_copy(n, device, t))
    join(across_q)
    join(far_q)
    for n, device in ((6, across), (7, far), (8, partner)):
        stat_copy(n, device, device[1]).wait_recv()
    total = stats[0]
    for i in range(1, tp_ways):
        total = total + stats[i]
    total = jnp.concatenate([total, jnp.zeros((120, tok), F32)], axis=0).T
    channels = saved.shape[1] * tp_ways
    mean_one = total[:, 0:1] / channels
    mean_two = total[:, 1:2] / channels
    std = jnp.broadcast_to(std_ref[...], (tok, tok)).T[:, 0:1]
    conv = std * (norm_grad - mean_one - saved * mean_two)
    ext[pl.ds(0, tok), :] = conv

    def halo_copy():
        return remote(ext.at[pl.ds(0, 32)], ext.at[pl.ds(tok, 32)], t_send.at[9], t_recv.at[9], before)

    @pl.when(s > 0)
    def _():
        halo_copy().start()

    fill(len(items))

    @pl.when(s < sp_ways - 1)
    def _():
        halo_copy().wait_recv()

    @pl.when(s == sp_ways - 1)
    def _():
        ext[pl.ds(tok, 32), :] = jnp.zeros((32, ext.shape[1]), F32)

    glu = taps_ref[0:1, :] * ext[pl.ds(0, tok), :]
    for k in range(1, ksize):
        glu = glu + taps_ref[k : k + 1, :] * ext[pl.ds(k, tok), :]
    in_sig = jax.nn.sigmoid(gate_ref[...].astype(F32))
    vgrad_ref[...] = (glu * in_sig).astype(BF16)
    ggrad_ref[...] = (glu * value_ref[...].astype(F32) * in_sig * (1.0 - in_sig)).astype(BF16)

    def q_arrival(j):
        plane = planes[j]
        return remote(pz_out.at[plane], pz.at[plane], q_send.at[plane], q_recv.at[plane], z_peers[j - 1])

    total = pgrad_ref[...]
    for j in range(1, experts):
        q_arrival(j).wait_recv()
        total = total + pz[planes[j]].astype(F32)
    pgrad_ref[...] = total

    @pl.when(s > 0)
    def _():
        halo_copy().wait_send()

    for copy in sent + [q_arrival(j) for j in range(1, experts)]:
        copy.wait_send()


def mega(hidden, cot, routes, weights, w_gate, w_up, w_down, value, gate_in, normed, std, gain, taps, w_proj, experts, cap, tp_ways):
    vmem = pl.BlockSpec(memory_space=pltpu.VMEM)
    hbm = pl.BlockSpec(memory_space=pl.ANY)
    tok, width = cot.shape
    units = w_gate.shape[0]
    quarter = width // tp_ways
    padded = -(-experts // 8) * 8
    total = experts * GROUP * cap
    ch = normed.shape[1]
    rows = width // (experts * GROUP)
    half = quarter // 2
    dma = pltpu.SemaphoreType.DMA
    arrays = (hidden, cot, routes, weights, w_gate, w_up, w_down, value, gate_in, normed, std, gain, taps, w_proj)
    assert taps.shape[0] - 1 <= 32
    return pl.pallas_call(
        functools.partial(mega_kernel, experts, cap, taps.shape[0]),
        out_shape=(
            pltpu.VMEM((units, width), BF16),
            pltpu.VMEM((units, width), BF16),
            pltpu.VMEM((units, width), BF16),
            pltpu.VMEM((tok, quarter), BF16),
            pltpu.VMEM((rows, ch), F32),
            pltpu.VMEM((tok, ch), BF16),
            pltpu.VMEM((tok, ch), BF16),
        ),
        in_specs=[hbm] * len(arrays),
        out_specs=(vmem,) * 7,
        scratch_shapes=[
            pltpu.VMEM((tok, width), BF16),
            pltpu.VMEM((tok, width), BF16),
            *[pltpu.VMEM(a.shape, a.dtype) for a in (routes, weights, value, gate_in, normed, std, gain, taps, w_proj)],
            pltpu.VMEM((padded, tok), jnp.int32),
            pltpu.VMEM((padded, tok), F32),
            pltpu.VMEM((2, total, width), BF16),
            pltpu.VMEM((experts, 2, cap, quarter), BF16),
            pltpu.VMEM((units, width), BF16),
            pltpu.VMEM((units, width), BF16),
            pltpu.VMEM((units, width), BF16),
            pltpu.VMEM((total, units), BF16),
            pltpu.VMEM((total, units), BF16),
            pltpu.VMEM((total, units), BF16),
            pltpu.VMEM((2 * units, total), BF16),
            pltpu.VMEM((total, width), BF16),
            pltpu.VMEM((experts, PAIR, GROUP * cap, quarter), BF16),
            pltpu.VMEM((2, experts, PAIR, GROUP, cap, half), BF16),
            pltpu.VMEM((experts, GROUP, cap, half), BF16),
            pltpu.VMEM((experts, PAIR, cap, half), BF16),
            pltpu.VMEM((2, experts, cap, half), BF16),
            pltpu.VMEM((2, experts, cap, half), BF16),
            pltpu.VMEM((experts, cap, quarter), BF16),
            pltpu.VMEM((experts, cap, quarter), BF16),
            pltpu.VMEM((tok, width), BF16),
            pltpu.VMEM((tp_ways, 8, tok), F32),
            pltpu.VMEM((tok + 32, ch), F32),
            pltpu.VMEM((experts, GROUP, rows, ch), BF16),
            pltpu.VMEM((experts, rows, ch), BF16),
            pltpu.VMEM((experts, rows, ch), BF16),
            pltpu.VMEM((experts, rows, ch), BF16),
            dma((4,)),
            dma((3,)),
            dma((7,)),
            dma((experts, 2, 2, 2)),
            dma((experts, 2, 2, 2)),
            dma((experts, 2, 2)),
            dma((experts, 2, 2)),
            dma((experts, PAIR)),
            dma((experts, PAIR)),
            dma((experts, 4)),
            dma((experts, 4)),
            dma((experts,)),
            dma((experts,)),
            dma((10,)),
            dma((10,)),
            dma((experts,)),
            dma((experts,)),
            dma((experts,)),
            dma((experts,)),
        ],
        compiler_params=pltpu.CompilerParams(
            collective_id=0, has_side_effects=True, vmem_limit_bytes=44 * 1024 * 1024
        ),
        name="mega",
    )(*[pltpu.with_memory_space_constraint(a, pltpu.HBM) for a in arrays])


def finish_kernel(count, *refs):
    copies = [pltpu.make_async_copy(refs[n], refs[count + n], refs[-1].at[n]) for n in range(count)]
    for copy in copies:
        copy.start()
    for copy in copies:
        copy.wait()


def finish(*arrays):
    count = len(arrays)
    return pl.pallas_call(
        functools.partial(finish_kernel, count),
        out_shape=tuple(jax.ShapeDtypeStruct(a.shape, a.dtype) for a in arrays),
        in_specs=[pl.BlockSpec(memory_space=pltpu.VMEM)] * count,
        out_specs=(pl.BlockSpec(memory_space=pl.ANY),) * count,
        scratch_shapes=[pltpu.SemaphoreType.DMA((count,))],
        compiler_params=pltpu.CompilerParams(vmem_limit_bytes=8 * 1024 * 1024),
        name="finish",
    )(*[pltpu.with_memory_space_constraint(a, pltpu.VMEM) for a in arrays])


def on_device(
    hidden_state, out_grad, routes, route_weights, w_gate, w_up, w_down,
    value, gate_in, normed, inv_std, norm_gain, taps, w_proj,
):
    tok = hidden_state.shape[0]
    top_k = routes.shape[1]
    sp_ways, tp_ways = lax.axis_size("sp"), lax.axis_size("tp")
    experts = sp_ways // GROUP
    cap = 3 * tok * top_k // (2 * experts)
    cap = -(-cap // 16) * 16
    results = mega(
        hidden_state, out_grad, routes.T, route_weights.T, w_gate[0].T, w_up[0].T, w_down[0], value, gate_in, normed,
        inv_std[None, :], norm_gain[None, :], taps, w_proj, experts, cap, tp_ways,
    )
    gate_wgrad, up_wgrad, down_grad, stream_part, proj_grad, value_grad, gate_in_grad = finish(*results)
    return gate_wgrad.T[None], up_wgrad.T[None], down_grad[None], stream_part, proj_grad, value_grad, gate_in_grad


def solution(mesh):
    in_specs = (
        P("sp", None), P("sp", None), P("sp", None), P("sp", None),
        P("sp", None, "tp"), P("sp", None, "tp"), P("sp", "tp", None),
        P("sp", "tp"), P("sp", "tp"), P("sp", "tp"), P("sp"), P("tp"), P(None, "tp"), P(None, "tp"),
    )
    out_specs = (
        P("sp", None, "tp"), P("sp", None, "tp"), P("sp", "tp", None),
        P("sp", "tp"), P("sp", "tp"), P("sp", "tp"), P("sp", "tp"),
    )
    return jax.shard_map(on_device, mesh=mesh, in_specs=in_specs, out_specs=out_specs, check_vma=False)
```

```python
import functools

import jax
import jax.numpy as jnp
from jax import lax
from jax.experimental import pallas as pl
from jax.experimental.pallas import tpu as pltpu
from jax.sharding import PartitionSpec as P

GROUP = 2
PAIR = 2
MESH = pl.DeviceIdType.MESH
F32 = jnp.float32
BF16 = jnp.bfloat16


def dot_rows(a, b):
    return lax.dot_general(a, b, (((0,), (0,)), ((), ())), preferred_element_type=F32)


def dot_cols(a, b):
    return lax.dot_general(a, b, (((1,), (1,)), ((), ())), preferred_element_type=F32)


def place():
    s, t = lax.axis_index("sp"), lax.axis_index("tp")
    e, g = s // GROUP, s % GROUP
    hi, lo = t // PAIR, t % PAIR
    across = (s, (1 - hi) * PAIR + lo)
    beside = (e * GROUP + 1 - g, t)
    partner = (s, hi * PAIR + 1 - lo)
    return s, t, e, g, hi, lo, across, beside, partner


def flip(place, bits):
    bit = 1
    while bit <= bits:
        if bits & bit:
            place = place + bit - 2 * bit * lax.rem(place // bit, 2)
        bit *= 2
    return place


def hail(devices):
    for device in devices:
        pl.semaphore_signal(pltpu.get_barrier_semaphore(), inc=1, device_id=device, device_id_type=MESH)


def greet(devices):
    pl.semaphore_wait(pltpu.get_barrier_semaphore(), len(devices))


def remote(src, dst, send, recv, device):
    return pltpu.make_async_remote_copy(
        src_ref=src, dst_ref=dst, send_sem=send, recv_sem=recv, device_id=device, device_id_type=MESH
    )


def one_hot(rank_row, cap):
    slots = lax.broadcasted_iota(jnp.int32, (cap, rank_row.shape[1]), 0)
    return jnp.where(slots == rank_row, 1.0, 0.0)


def rank_tokens(routes_ref, weights_ref, rank_ref, w_ref):
    top, tok = routes_ref.shape
    experts = lax.broadcasted_iota(jnp.int32, rank_ref.shape, 0)
    named = jnp.zeros(rank_ref.shape, F32)
    weight = jnp.zeros(rank_ref.shape, F32)
    for k in range(top):
        hit = routes_ref[k : k + 1, :] == experts
        named = jnp.where(hit, 1.0, named)
        weight = jnp.where(hit, weights_ref[k : k + 1, :], weight)
    first = lax.broadcasted_iota(jnp.int32, (tok, tok), 0)
    second = lax.broadcasted_iota(jnp.int32, (tok, tok), 1)
    earlier = jnp.where(first < second, 1.0, 0.0).astype(BF16)
    rank = jnp.dot(named.astype(BF16), earlier, preferred_element_type=F32)
    rank_ref[...] = jnp.where(named > 0.0, rank, -1.0).astype(jnp.int32)
    w_ref[...] = weight


def mega_kernel(
    experts, cap, ksize,
    h_hbm, cot_hbm, routes_hbm, weights_hbm, gate_hbm, up_hbm, down_hbm,
    value_hbm, gin_hbm, normed_hbm, std_hbm, gain_hbm, taps_hbm, proj_hbm,
    gw, uw, dw, stream_ref, pgrad_ref, vgrad_ref, ggrad_ref,
    h_ref, cot_ref, routes_ref, weights_ref, value_ref, gate_ref, normed_ref, std_ref, gain_ref, taps_ref, proj_ref,
    rank_ref, w_ref, buf, pack, wg, wu, wd, act, gg, ug, flipped, grad_ref,
    from_core, sums, rx_a, ry_b, relay, rx2, back, done, full, stats, ext, pg, py, pz_out, pz,
    h_sem, w_sem, x_sem, l_send, l_recv, c_send, c_recv,
    core_send, core_recv, hop_send, hop_recv, z_send, z_recv, t_send, t_recv, p_send, p_recv, q_send, q_recv,
):
    s, t, e, g, hi, lo, across, beside, partner = place()
    sp_ways = experts * GROUP
    tp_ways = stats.shape[0]
    tok, quarter = cot_ref.shape[0], cot_ref.shape[1] // tp_ways
    half = quarter // 2
    across_t, other_t = across[1], partner[1]
    far_t = (1 - hi) * PAIR + 1 - lo
    far = (s, far_t)
    planes = [flip(e, j) for j in range(experts)]
    z_peers = [(planes[j] * GROUP + g, t) for j in range(1, experts)]
    before = (lax.rem(s + sp_ways - 1, sp_ways), t)
    after = (lax.rem(s + 1, sp_ways), t)
    friends = z_peers + [across, beside, partner, far, before, after]
    hail(friends)
    def fetch(sem, *pairs):
        return [pltpu.make_async_copy(src, dst, sem.at[n]) for n, (src, dst) in enumerate(pairs)]

    takes = fetch(
        h_sem, (routes_hbm, routes_ref), (weights_hbm, weights_ref),
        (h_hbm, h_ref), (cot_hbm, cot_ref),
    )
    loads = fetch(w_sem, (gate_hbm, wg), (up_hbm, wu), (down_hbm, wd))
    extras = fetch(
        x_sem, (normed_hbm, normed_ref), (gain_hbm, gain_ref), (proj_hbm, proj_ref), (std_hbm, std_ref),
        (taps_hbm, taps_ref), (gin_hbm, gate_ref), (value_hbm, value_ref),
    )
    for copy in takes:
        copy.start()
    for copy in takes[:2]:
        copy.wait()
    rank_tokens(routes_ref, weights_ref, rank_ref, w_ref)
    for copy in takes[2:]:
        copy.wait()
    for copy in loads + extras:
        copy.start()
    sent = []

    def go(copy):
        copy.start()
        sent.append(copy)

    def cols_of(col):
        return pl.ds(pl.multiple_of(col * quarter, quarter), quarter)

    def rows_of(j):
        return pl.ds(pl.multiple_of(j * GROUP * cap, cap), GROUP * cap)

    def loc(j, side, col):
        return pl.ds(pl.multiple_of((j * GROUP + side) * cap, cap), cap), cols_of(col)

    def chosen(j):
        plane = pl.ds(planes[j], 1)
        hot = one_hot(rank_ref[plane, :], cap)
        return hot.astype(BF16), jnp.sum(hot * w_ref[plane, :], axis=1, keepdims=True)

    sides = (g, 1 - g)
    spread = (t, across_t)

    def spot(k, j, side, col):
        rows, cols = loc(j, sides[side], spread[col])
        return buf.at[k, rows, cols]

    def link(k, j, side, col, src, dst, device):
        return remote(src, dst, l_send.at[j, k, side, col], l_recv.at[j, k, side, col], device)

    def landed(k, j, side, col):
        ref = spot(k, j, side, col)
        link(k, j, side, col, ref, ref, partner).wait_recv()

    def pass_on(k, j, side, col, src, device):
        ref = spot(k, j, *src)
        go(link(k, j, side, col, ref, ref, device))

    def core(j, side, col):
        rows, cols = loc(j, sides[side], spread[col])
        ref = buf.at[:, rows, cols]
        return remote(ref, ref, c_send.at[j, side, col], c_recv.at[j, side, col], partner)

    def core_landed(j, side, col):
        rows, cols = loc(j, sides[side], (other_t, far_t)[col])
        ref = buf.at[:, rows, cols]
        remote(ref, ref, c_send.at[j, side, col], c_recv.at[j, side, col], partner).wait_recv()

    step = max(1, experts // 4)
    blocks = [list(range(c, min(c + step, experts))) for c in range(0, experts, step)]
    first_block, last_blocks = blocks[1], blocks[:1:-1]
    outer = [j for block in [first_block] + last_blocks + blocks[:1] for j in block if j]

    def z_out(k, j):
        return link(k, j, 0, 0, pack.at[j, k], spot(k, j, 0, 0), z_peers[j - 1])

    def z_start(block):
        for j in block:
            for k in range(2):
                z_out(k, j).start()

    far_one, far_two = last_blocks
    rest = blocks[0][1:]
    middle = (lax.rem(e, 4) + 1) // 2 == 1
    for j in outer:
        hot, scale = chosen(j)
        pack[j, 0] = jnp.dot(hot, h_ref[:, cols_of(t)], preferred_element_type=F32).astype(BF16)
        pack[j, 1] = (jnp.dot(hot, cot_ref[:, cols_of(t)], preferred_element_type=F32) * scale).astype(BF16)
        sent.extend(z_out(k, j) for k in range(2))
        if j == first_block[-1]:
            greet(friends)
            z_start(first_block)

    @pl.when(middle)
    def _():
        z_start(far_one + far_two + rest)

    hot, scale = chosen(0)
    here = loc(0, g, t)[0]
    buf[0, here, :] = jnp.dot(hot, h_ref[...], preferred_element_type=F32).astype(BF16)
    buf[1, here, :] = (jnp.dot(hot, cot_ref[...], preferred_element_type=F32) * scale).astype(BF16)

    def d_first(j):
        for k in range(2):
            if j:
                landed(k, j, 0, 0)
                pass_on(k, j, 0, 1, (0, 0), across)
            pass_on(k, j, 1, 0, (0, 0), beside)
        if j:
            go(core(j, 0, 0))

    def d_second(j):
        if j:
            landed(0, j, 0, 1)
            pass_on(0, j, 1, 1, (0, 1), beside)
            landed(1, j, 1, 0)
            pass_on(1, j, 1, 1, (1, 0), across)
            landed(1, j, 0, 1)
            go(core(j, 0, 1))
            landed(0, j, 1, 0)
        else:
            for k in range(2):
                landed(k, j, 1, 0)
                pass_on(k, j, 1, 1, (1, 0), across)
        go(core(j, 1, 0))

    def d_third(j):
        for k in range(2):
            landed(k, j, 1, 1)
        go(core(j, 1, 1))

    def d_last(j):
        for side in range(0 if j else 1, 2):
            for col in range(2):
                core_landed(j, side, col)

    def compute(j):
        rows = rows_of(j)
        in_rows = buf[0, rows, :]
        in_cots = buf[1, rows, :]
        pre_gate = dot_cols(in_rows, wg[...])
        pre_up = dot_cols(in_rows, wu[...])
        gate_sig = jax.nn.sigmoid(pre_gate)
        silu_gate = pre_gate * gate_sig
        act_grad = dot_cols(in_cots, wd[...])
        gate_grad = (act_grad * pre_up * gate_sig * (1.0 + pre_gate * (1.0 - gate_sig))).astype(BF16)
        up_grad = (act_grad * silu_gate).astype(BF16)
        act[rows, :] = (silu_gate * pre_up).astype(BF16)
        gg[rows, :] = gate_grad
        ug[rows, :] = up_grad

    def compute_back(j):
        rows = rows_of(j)
        gate_grad, up_grad = gg[rows, :], ug[rows, :]
        for lane in (1 - lo, lo):
            for h in range(PAIR):
                cols = cols_of(lane * PAIR + h)
                grad_ref[rows, cols] = (
                    jnp.dot(gate_grad, wg[:, cols], preferred_element_type=F32)
                    + jnp.dot(up_grad, wu[:, cols], preferred_element_type=F32)
                ).astype(BF16)
                if lane is not lo and isinstance(j, int):
                    go(core_copy(j, h, 1 - lo))

    width = full.shape[1]
    piece = 256
    per_item = width // piece // 8
    units = gw.shape[0]

    def weight_item(which, n):
        if which == 0:
            if n == 0:
                flipped[pl.ds(0, units), :] = gg[...].T
                flipped[pl.ds(units, units), :] = ug[...].T

            @pl.loop(n * per_item, (n + 1) * per_item)
            def _(i):
                cols = pl.ds(pl.multiple_of(i * piece, piece), piece)
                both_grads = jnp.dot(flipped[...], buf[0, :, cols], preferred_element_type=F32).astype(BF16)
                gw[:, cols] = both_grads[:units]
                uw[:, cols] = both_grads[units:]
        else:
            if n == 0:
                flipped[pl.ds(0, units), :] = act[...].T

            @pl.loop(2 * n * per_item, 2 * (n + 1) * per_item)
            def _(i):
                cols = pl.ds(pl.multiple_of(i * piece, piece), piece)
                dw[:, cols] = jnp.dot(
                    flipped[pl.ds(0, units), :], buf[1, :, cols], preferred_element_type=F32
                ).astype(BF16)

    items = [(0, n) for n in range(8)] + [(1, n) for n in range(4)]

    def fill(count=1):
        for _ in range(count):
            if items:
                weight_item(*items.pop(0))

    def core_copy(j, h, lane):
        return remote(
            grad_ref.at[rows_of(j), cols_of(lane * PAIR + h)],
            from_core.at[j, h], core_send.at[j, h], core_recv.at[j, h], partner,
        )

    def hop_copy(n, j, src, dst, device):
        return remote(src, dst, hop_send.at[j, n], hop_recv.at[j, n], device)

    def x_first(j):
        return hop_copy(0, j, sums.at[0, j, 1 - hi], rx_a.at[j], across)

    def y_first(j):
        return hop_copy(1, j, sums.at[1, j, :, 1 - g], ry_b.at[j], beside)

    def y_second(j):
        return hop_copy(2, j, relay.at[0, j], rx2.at[0, j], beside)

    def x_second(j):
        return hop_copy(3, j, relay.at[1, j], rx2.at[1, j], across)

    def z_copy(j):
        return remote(done.at[j], back.at[j], z_send.at[j], z_recv.at[j], z_peers[j - 1])

    def first(j):
        for h in range(PAIR):
            core_copy(j, h, lo).wait_recv()
            mine = grad_ref[rows_of(j), cols_of(lo * PAIR + h)].astype(F32)
            total = (mine + from_core[j, h].astype(F32)).astype(BF16).reshape(GROUP, cap, quarter)
            sums[0, j, h] = total[:, :, :half]
            sums[1, j, h] = total[:, :, half:]
        go(x_first(j))
        go(y_first(j))

    def second(j):
        x_first(j).wait_recv()
        relay[0, j] = (sums[0, j, hi, 1 - g].astype(F32) + rx_a[j, 1 - g].astype(F32)).astype(BF16)
        go(y_second(j))
        y_first(j).wait_recv()
        relay[1, j] = (sums[1, j, 1 - hi, g].astype(F32) + ry_b[j, 1 - hi].astype(F32)).astype(BF16)
        go(x_second(j))

    def third(j):
        y_second(j).wait_recv()
        done[j, :, :half] = (
            sums[0, j, hi, g].astype(F32) + rx_a[j, g].astype(F32) + rx2[0, j].astype(F32)
        ).astype(BF16)
        x_second(j).wait_recv()
        done[j, :, half:] = (
            sums[1, j, hi, g].astype(F32) + ry_b[j, hi].astype(F32) + rx2[1, j].astype(F32)
        ).astype(BF16)
        if j:
            go(z_copy(j))

    def flow(*stages):
        for stage, block in stages:
            for j in block:
                stage(j)

    def work(block, *stages):
        for stage in stages:
            if len(block) == 1:
                stage(block[0])
            else:
                pl.loop(block[0], block[-1] + 1)(stage)
        if len(block) > 1 and compute_back in stages:
            for j in block:
                for h in range(PAIR):
                    go(core_copy(j, h, 1 - lo))

    own, near = blocks[0], first_block
    d_first(0)
    flow((d_first, near))

    flow((d_second, [0]))

    @pl.when(jnp.logical_not(middle))
    def _():
        z_start(far_one + far_two + rest)

    flow((d_second, near), (d_first, far_one))
    flow((d_third, near), (d_third, [0]))
    flow((d_last, near), (d_first, far_two))
    for copy in loads:
        copy.wait()
    work(near, compute, compute_back)
    flow((d_second, far_one), (d_first, rest), (d_second, rest), (d_third, rest), (d_last, own))
    work(own, compute, compute_back)
    flow((d_second, far_two), (first, near))
    flow((d_third, far_one), (d_last, far_one), (first, own))
    work(far_one, compute, compute_back)
    flow((d_third, far_two), (first, far_one), (d_last, far_two), (second, near))
    work(far_two, compute)
    flow((second, own))
    work(far_two, compute_back)
    flow((second, far_one), (first, far_two), (third, near), (third, own))
    fill(2)
    flow((third, far_one))
    fill(2)
    flow((second, far_two))
    fill(2)
    flow((third, far_two))
    fill(5)

    for copy in extras:
        copy.wait()
    gain = gain_ref[...]
    saved = normed_ref[...].astype(F32)
    pre_act = saved * gain
    act_sig = jax.nn.sigmoid(pre_act)
    slope = act_sig * (1.0 + pre_act * (1.0 - act_sig))
    proj_act = (pre_act * act_sig).astype(BF16)

    own_q, other_q = lo * PAIR + hi, (1 - lo) * PAIR + hi
    across_q, far_q = lo * PAIR + 1 - hi, (1 - lo) * PAIR + 1 - hi
    stream = cot_ref[:, cols_of(own_q)].astype(F32)
    for j in [0] + [k for block in (near, far_one, far_two, own[1:]) for k in block]:
        if j:
            z_copy(j).wait_recv()
            block = back[j]
        else:
            block = done[0]
        hot = one_hot(rank_ref[pl.ds(planes[j], 1), :], cap).astype(BF16)
        stream = stream + dot_rows(hot, block)
    full[:, cols_of(own_q)] = stream.astype(BF16)

    def strip(col, n):
        return pl.ds(pl.multiple_of(col * quarter + seq[n] * half, half), half)

    def gather_copy(n, k, col, device):
        ref = full.at[:, strip(col, n)]
        return remote(ref, ref, t_send.at[2 * k + n], t_recv.at[2 * k + n], device)

    rows = pg.shape[2]
    share = experts // tp_ways
    seq = (1 - g, g) if share == 1 else (0, 1)

    def p_copy(plane):
        return remote(pg.at[plane, 1 - g], py.at[plane], p_send.at[plane], p_recv.at[plane], beside)

    def q_copy(plane):
        return remote(pz_out.at[plane], pz.at[e], q_send.at[plane], q_recv.at[e], (plane * GROUP + g, t))

    def part(col, n):
        block = full[:, strip(col, n)]
        pall = dot_rows(block, proj_act).astype(BF16)
        if share == 1:
            pg[col, seq[n]] = pall
            planes_here = [col] * (1 - n)
        else:
            pall = pall.reshape(share // 2, GROUP, rows, proj_act.shape[1])
            planes_here = [col * share + n * (share // 2) + m for m in range(share // 2)]
            for m, plane in enumerate(planes_here):
                pg[plane] = pall[m]
        for plane in planes_here:
            go(p_copy(plane))
        return jnp.dot(block, proj_ref[strip(col, n), :], preferred_element_type=F32)

    def join(col):
        for n in range(share):
            plane = col * share + n
            p_copy(plane).wait_recv()
            piece = pg[plane, g].astype(F32) + py[plane].astype(F32)
            pz_out[plane] = piece.astype(BF16)

            @pl.when(plane == e)
            def _():
                pgrad_ref[...] = piece

            @pl.when(plane != e)
            def _():
                q_copy(plane).start()

    for n in range(2):
        go(gather_copy(n, 0, own_q, across))
        go(gather_copy(n, 1, own_q, partner))
    proj_in = part(own_q, 0) + part(own_q, 1)
    fill(1)
    for n in range(2):
        gather_copy(n, 1, other_q, partner).wait_recv()
        proj_in = proj_in + part(other_q, n)
    for n in range(2):
        gather_copy(n, 0, across_q, across).wait_recv()
        go(gather_copy(n, 2, across_q, partner))
        proj_in = proj_in + part(across_q, n)
        join((own_q, other_q)[n])
        gather_copy(n, 2, far_q, partner).wait_recv()
        proj_in = proj_in + part(far_q, n)
    stream_ref[...] = full[:, cols_of(t)]
    norm_grad = proj_in * slope * gain
    one = jnp.sum(norm_grad, axis=1, keepdims=True)
    two = jnp.sum(norm_grad * saved, axis=1, keepdims=True)
    lane = lax.broadcasted_iota(jnp.int32, (tok, 128), 1)
    packed = jnp.where(lane == 0, one, jnp.where(lane == 1, two, 0.0))
    stats[t] = packed.T[:8]

    def stat_copy(n, device, owner):
        return remote(stats.at[owner], stats.at[owner], t_send.at[n], t_recv.at[n], device)

    for n, device in ((6, across), (7, far), (8, partner)):
        go(stat_copy(n, device, t))
    join(across_q)
    join(far_q)
    for n, device in ((6, across), (7, far), (8, partner)):
        stat_copy(n, device, device[1]).wait_recv()
    total = stats[0]
    for i in range(1, tp_ways):
        total = total + stats[i]
    total = jnp.concatenate([total, jnp.zeros((120, tok), F32)], axis=0).T
    channels = saved.shape[1] * tp_ways
    mean_one = total[:, 0:1] / channels
    mean_two = total[:, 1:2] / channels
    std = jnp.broadcast_to(std_ref[...], (tok, tok)).T[:, 0:1]
    conv = std * (norm_grad - mean_one - saved * mean_two)
    ext[pl.ds(0, tok), :] = conv

    def halo_copy():
        return remote(ext.at[pl.ds(0, 32)], ext.at[pl.ds(tok, 32)], t_send.at[9], t_recv.at[9], before)

    @pl.when(s > 0)
    def _():
        halo_copy().start()

    fill(len(items))

    @pl.when(s < sp_ways - 1)
    def _():
        halo_copy().wait_recv()

    @pl.when(s == sp_ways - 1)
    def _():
        ext[pl.ds(tok, 32), :] = jnp.zeros((32, ext.shape[1]), F32)

    glu = taps_ref[0:1, :] * ext[pl.ds(0, tok), :]
    for k in range(1, ksize):
        glu = glu + taps_ref[k : k + 1, :] * ext[pl.ds(k, tok), :]
    in_sig = jax.nn.sigmoid(gate_ref[...].astype(F32))
    vgrad_ref[...] = (glu * in_sig).astype(BF16)
    ggrad_ref[...] = (glu * value_ref[...].astype(F32) * in_sig * (1.0 - in_sig)).astype(BF16)

    def q_arrival(j):
        plane = planes[j]
        return remote(pz_out.at[plane], pz.at[plane], q_send.at[plane], q_recv.at[plane], z_peers[j - 1])

    total = pgrad_ref[...]
    for j in range(1, experts):
        q_arrival(j).wait_recv()
        total = total + pz[planes[j]].astype(F32)
    pgrad_ref[...] = total

    @pl.when(s > 0)
    def _():
        halo_copy().wait_send()

    for copy in sent + [q_arrival(j) for j in range(1, experts)]:
        copy.wait_send()


def mega(hidden, cot, routes, weights, w_gate, w_up, w_down, value, gate_in, normed, std, gain, taps, w_proj, experts, cap, tp_ways):
    vmem = pl.BlockSpec(memory_space=pltpu.VMEM)
    hbm = pl.BlockSpec(memory_space=pl.ANY)
    tok, width = cot.shape
    units = w_gate.shape[0]
    quarter = width // tp_ways
    padded = -(-experts // 8) * 8
    total = experts * GROUP * cap
    ch = normed.shape[1]
    rows = width // (experts * GROUP)
    half = quarter // 2
    dma = pltpu.SemaphoreType.DMA
    arrays = (hidden, cot, routes, weights, w_gate, w_up, w_down, value, gate_in, normed, std, gain, taps, w_proj)
    assert taps.shape[0] - 1 <= 32
    return pl.pallas_call(
        functools.partial(mega_kernel, experts, cap, taps.shape[0]),
        out_shape=(
            pltpu.VMEM((units, width), BF16),
            pltpu.VMEM((units, width), BF16),
            pltpu.VMEM((units, width), BF16),
            pltpu.VMEM((tok, quarter), BF16),
            pltpu.VMEM((rows, ch), F32),
            pltpu.VMEM((tok, ch), BF16),
            pltpu.VMEM((tok, ch), BF16),
        ),
        in_specs=[hbm] * len(arrays),
        out_specs=(vmem,) * 7,
        scratch_shapes=[
            pltpu.VMEM((tok, width), BF16),
            pltpu.VMEM((tok, width), BF16),
            *[pltpu.VMEM(a.shape, a.dtype) for a in (routes, weights, value, gate_in, normed, std, gain, taps, w_proj)],
            pltpu.VMEM((padded, tok), jnp.int32),
            pltpu.VMEM((padded, tok), F32),
            pltpu.VMEM((2, total, width), BF16),
            pltpu.VMEM((experts, 2, cap, quarter), BF16),
            pltpu.VMEM((units, width), BF16),
            pltpu.VMEM((units, width), BF16),
            pltpu.VMEM((units, width), BF16),
            pltpu.VMEM((total, units), BF16),
            pltpu.VMEM((total, units), BF16),
            pltpu.VMEM((total, units), BF16),
            pltpu.VMEM((2 * units, total), BF16),
            pltpu.VMEM((total, width), BF16),
            pltpu.VMEM((experts, PAIR, GROUP * cap, quarter), BF16),
            pltpu.VMEM((2, experts, PAIR, GROUP, cap, half), BF16),
            pltpu.VMEM((experts, GROUP, cap, half), BF16),
            pltpu.VMEM((experts, PAIR, cap, half), BF16),
            pltpu.VMEM((2, experts, cap, half), BF16),
            pltpu.VMEM((2, experts, cap, half), BF16),
            pltpu.VMEM((experts, cap, quarter), BF16),
            pltpu.VMEM((experts, cap, quarter), BF16),
            pltpu.VMEM((tok, width), BF16),
            pltpu.VMEM((tp_ways, 8, tok), F32),
            pltpu.VMEM((tok + 32, ch), F32),
            pltpu.VMEM((experts, GROUP, rows, ch), BF16),
            pltpu.VMEM((experts, rows, ch), BF16),
            pltpu.VMEM((experts, rows, ch), BF16),
            pltpu.VMEM((experts, rows, ch), BF16),
            dma((4,)),
            dma((3,)),
            dma((7,)),
            dma((experts, 2, 2, 2)),
            dma((experts, 2, 2, 2)),
            dma((experts, 2, 2)),
            dma((experts, 2, 2)),
            dma((experts, PAIR)),
            dma((experts, PAIR)),
            dma((experts, 4)),
            dma((experts, 4)),
            dma((experts,)),
            dma((experts,)),
            dma((10,)),
            dma((10,)),
            dma((experts,)),
            dma((experts,)),
            dma((experts,)),
            dma((experts,)),
        ],
        compiler_params=pltpu.CompilerParams(
            collective_id=0, has_side_effects=True, vmem_limit_bytes=44 * 1024 * 1024
        ),
        name="mega",
    )(*[pltpu.with_memory_space_constraint(a, pltpu.HBM) for a in arrays])


def finish_kernel(count, *refs):
    copies = [pltpu.make_async_copy(refs[n], refs[count + n], refs[-1].at[n]) for n in range(count)]
    for copy in copies:
        copy.start()
    for copy in copies:
        copy.wait()


def finish(*arrays):
    count = len(arrays)
    return pl.pallas_call(
        functools.partial(finish_kernel, count),
        out_shape=tuple(jax.ShapeDtypeStruct(a.shape, a.dtype) for a in arrays),
        in_specs=[pl.BlockSpec(memory_space=pltpu.VMEM)] * count,
        out_specs=(pl.BlockSpec(memory_space=pl.ANY),) * count,
        scratch_shapes=[pltpu.SemaphoreType.DMA((count,))],
        compiler_params=pltpu.CompilerParams(vmem_limit_bytes=8 * 1024 * 1024),
        name="finish",
    )(*[pltpu.with_memory_space_constraint(a, pltpu.VMEM) for a in arrays])


def on_device(
    hidden_state, out_grad, routes, route_weights, w_gate, w_up, w_down,
    value, gate_in, normed, inv_std, norm_gain, taps, w_proj,
):
    tok = hidden_state.shape[0]
    top_k = routes.shape[1]
    sp_ways, tp_ways = lax.axis_size("sp"), lax.axis_size("tp")
    experts = sp_ways // GROUP
    cap = 3 * tok * top_k // (2 * experts)
    cap = -(-cap // 16) * 16
    results = mega(
        hidden_state, out_grad, routes.T, route_weights.T, w_gate[0].T, w_up[0].T, w_down[0], value, gate_in, normed,
        inv_std[None, :], norm_gain[None, :], taps, w_proj, experts, cap, tp_ways,
    )
    gate_wgrad, up_wgrad, down_grad, stream_part, proj_grad, value_grad, gate_in_grad = finish(*results)
    return gate_wgrad.T[None], up_wgrad.T[None], down_grad[None], stream_part, proj_grad, value_grad, gate_in_grad


def solution(mesh):
    in_specs = (
        P("sp", None), P("sp", None), P("sp", None), P("sp", None),
        P("sp", None, "tp"), P("sp", None, "tp"), P("sp", "tp", None),
        P("sp", "tp"), P("sp", "tp"), P("sp", "tp"), P("sp"), P("tp"), P(None, "tp"), P(None, "tp"),
    )
    out_specs = (
        P("sp", None, "tp"), P("sp", None, "tp"), P("sp", "tp", None),
        P("sp", "tp"), P("sp", "tp"), P("sp", "tp"), P("sp", "tp"),
    )
    return jax.shard_map(on_device, mesh=mesh, in_specs=in_specs, out_specs=out_specs, check_vma=False)
```
